32 devices in a mesh: sp: 8 (over z, y), tp: 4 (over x, core).
Axes of the slice: x: 2, y: 2, z: 4, core: 2. Of those that a mesh axis runs over, the one named last changes fastest.
Arguments:
- skip_stream_vector: bfloat16 [8192, 2048], P(('sp', 'tp')), may hold values from -6 to 6
- probe_preactivation: bfloat16 [8192, 1024], P('sp', 'tp'), may hold values from -6 to 6
- retention_preactivation: bfloat16 [8192, 1024], P('sp', 'tp'), may hold values from -4.5 to 4.5
- content_vector: bfloat16 [8192, 1024], P('sp', 'tp'), may hold values from -6 to 6
- emission_preactivation: bfloat16 [8192, 1024], P('sp', 'tp'), may hold values from -6 to 6
- retention_slack: float32 [1024], P('tp'), may hold values from 0 to 0.12
- surge_rate: float32 [8192, 1024], P('sp', 'tp'), may hold values from -1.2 to 0
- subspace_scaling_factor: float32 [1024], P('tp'), may hold values from 0.1 to 1.9
- emission_matrix: bfloat16 [1024, 2048], replicated, may hold values from -0.1875 to 0.1875
- mlp_scaling_factor: float32 [2048], replicated, may hold values from 0.1 to 1.9
- switch_matrix: bfloat16 [2048, 5632], P('sp', 'tp'), may hold values from -0.125 to 0.125
- expansion_matrix: bfloat16 [2048, 5632], P('sp', 'tp'), may hold values from -0.125 to 0.125
- contraction_matrix: bfloat16 [5632, 2048], P('tp', 'sp'), may hold values from -0.078125 to 0.078125
Outputs:
- stream_out: bfloat16 [8192, 2048], P(('sp', 'tp'))
The draws below stay inside these ranges and needn't reach their ends.
All inputs are finite; a program needn't handle non-finite values.
Results may differ from the reference program's by a relative error of at most 0.017.
Values may be sent and summed in bfloat16 or wider, within the bound.
No kernel may reach another device: no remote copies, remote signals or barrier semaphores. Data moves between devices by JAX's collectives and lax.ppermute only.
A program may use at most 128 MiB of HBM per device.

```python
import jax
import jax.numpy as jnp
from jax import lax

D = 2048
HEADS = 8
HEAD_DIM = 128
FF = 5632
BLOCK = 64
TOK_DEV = 1024
D_HGRN = 1024
TOKENS = 8192
N_TP = 4


def draw_retention_slack(key, part):
    first_key, second_key, third_key = jax.random.split(jax.random.fold_in(key, 11), 3)
    ranking = jax.random.permutation(first_key, HEADS)
    slow_heads = ranking < HEADS // 2
    slow_gap = jnp.exp(jax.random.uniform(second_key, (HEADS, HEAD_DIM), jnp.float32, jnp.log(0.2), jnp.log(0.8))) / TOKENS
    fast_gap = jnp.exp(jax.random.uniform(third_key, (HEADS, HEAD_DIM), jnp.float32, jnp.log(0.04), jnp.log(0.12)))
    chosen = jnp.where(slow_heads[:, None], slow_gap, fast_gap)
    return jnp.minimum(chosen, 0.12).reshape(HEADS * HEAD_DIM)


def draw_retention_preactivation(key, part):
    first_key, second_key = jax.random.split(jax.random.fold_in(key, 21))
    noise = jnp.clip(0.8 * jax.random.normal(first_key, (TOKENS, HEADS * HEAD_DIM), jnp.float32), -3.0, 3.0)
    offsets = jax.random.uniform(second_key, (TOKENS // TOK_DEV, HEADS), jnp.float32, -1.2, 1.2)
    spread_rows = jnp.repeat(jnp.repeat(offsets, TOK_DEV, axis=0), HEAD_DIM, axis=1)
    return (noise + spread_rows).astype(jnp.bfloat16)


def draw_surge_rate(key, part):
    first_key, second_key = jax.random.split(jax.random.fold_in(key, 31))
    positions = jax.random.randint(first_key, (2, HEADS), 0, TOKENS)
    strength = jnp.log(jax.random.uniform(second_key, (2, HEADS), jnp.float32, 0.55, 0.8))
    places = jnp.arange(TOKENS, dtype=jnp.int32)[:, None, None]
    hits = jnp.sum(jnp.where(places == positions[None, :, :], strength[None, :, :], 0.0), axis=1)
    return jnp.repeat(hits, HEAD_DIM, axis=1)


def levels(rng, shape, pieces, low, largest):
    loudness, own = 1.0, jax.random.fold_in(rng, 6)
    for position, shards_of in pieces:
        draws = jnp.exp(jax.random.uniform(jax.random.fold_in(own, position), (shards_of,), jnp.float32, low / len(pieces), largest / len(pieces)))
        loudness = loudness * jnp.repeat(draws, shape[position] // shards_of).reshape([-1 if axis == position else 1 for axis in range(len(shape))])
    return loudness


def normal_values(own_key, extent, width, limit, shards=(), kind=jnp.bfloat16):
    drawn = width * jax.random.normal(own_key, extent, jnp.float32)
    if shards:
        drawn = drawn * levels(own_key, extent, shards, -0.22, 0.18)
    return jnp.clip(drawn, -limit, limit).astype(kind)


def setup_inputs(seed: int = 0) -> dict:
    key_of = jax.random.split(jax.random.key(seed), 14)
    return {
        "skip_stream_vector": normal_values(key_of[0], (TOKENS, D), 1.0, 6.0, ((0, 32),)),
        "probe_preactivation": normal_values(key_of[1], (TOKENS, D_HGRN), 1.0, 6.0, ((0, 8), (1, 4))),
        "retention_preactivation": draw_retention_preactivation(jax.random.fold_in(key_of[13], 71), 0),
        "content_vector": normal_values(key_of[3], (TOKENS, D_HGRN), 1.0, 6.0, ((0, 8), (1, 4))),
        "emission_preactivation": normal_values(key_of[4], (TOKENS, D_HGRN), 1.0, 6.0, ((0, 8), (1, 4))),
        "retention_slack": draw_retention_slack(jax.random.fold_in(key_of[13], 71), 0),
        "surge_rate": draw_surge_rate(jax.random.fold_in(key_of[13], 71), 0),
        "subspace_scaling_factor": jnp.clip(1.0 + 0.18 * jax.random.normal(key_of[7], (D_HGRN,), jnp.float32), 0.1, 1.9),
        "emission_matrix": normal_values(key_of[8], (D_HGRN, D), D_HGRN ** -0.5, 0.1875),
        "mlp_scaling_factor": jnp.clip(1.0 + 0.18 * jax.random.normal(key_of[9], (D,), jnp.float32), 0.1, 1.9),
        "switch_matrix": normal_values(key_of[10], (D, FF), D ** -0.5, 0.125, ((0, 8), (1, 4))),
        "expansion_matrix": normal_values(key_of[11], (D, FF), D ** -0.5, 0.125, ((0, 8), (1, 4))),
        "contraction_matrix": normal_values(key_of[12], (FF, D), FF ** -0.5, 0.078125, ((0, 4), (1, 8))),
    }


EPSILON = 1e-06
TOP_PRECISION = lax.Precision.HIGHEST

def block_step(carry, inputs):
    memory_state, offsets = carry
    query_block, input_gate_block, value_block, log_blk = inputs
    cumulative_decay = jnp.cumsum(log_blk, axis=1)
    length = log_blk.shape[1]
    carried_share = jnp.einsum('eia,eax->eix', query_block * jnp.exp(cumulative_decay), memory_state, precision=TOP_PRECISION)
    middle = cumulative_decay[:, length // 2, :][:, None, :]
    left_side = query_block * jnp.exp(cumulative_decay - middle)
    right_side = input_gate_block * jnp.exp(middle - cumulative_decay)
    causal = (jnp.arange(length)[:, None] >= jnp.arange(length)[None, :])[None, :, :]
    scores = jnp.einsum('htk,hsk->hts', left_side, right_side, precision=TOP_PRECISION)
    scores = jnp.where(causal, scores, 0.0)
    outputs = carried_share + jnp.einsum('hts,hsv->htv', scores, value_block, precision=TOP_PRECISION)
    closing_log_decay = cumulative_decay[:, -1, :]
    updated_memory_state = jnp.exp(closing_log_decay)[:, :, None] * memory_state + jnp.einsum('qnj,qnl->qjl', input_gate_block * jnp.exp(closing_log_decay[:, None, :] - cumulative_decay), value_block, precision=TOP_PRECISION)
    return ((updated_memory_state, offsets + closing_log_decay), (outputs, cumulative_decay + offsets[:, None, :]))

def split_blocks(values, heads_here):
    count = values.shape[0]
    return values.reshape(count // BLOCK, BLOCK, heads_here, HEAD_DIM).transpose(0, 2, 1, 3)

def admission_source_matrix(probe_preactivation, retention_preactivation, content_vector, retention_slack, surge_rate):
    query_act = jax.nn.silu(probe_preactivation.astype(jnp.float32))
    admission_factor = retention_slack[None, :] * jax.nn.sigmoid(-retention_preactivation.astype(jnp.float32))
    retention_logarithm = jnp.log1p(-admission_factor) + surge_rate
    return (query_act, admission_factor, content_vector.astype(jnp.float32), retention_logarithm)

def head_output(outputs, subspace_scaling_factor, emission_preactivation):
    count, heads_here = (outputs.shape[0], outputs.shape[1])
    squares = lax.optimization_barrier(jnp.mean(outputs * outputs, axis=-1, keepdims=True))
    scaled = outputs * lax.rsqrt(squares + EPSILON) * subspace_scaling_factor.reshape(heads_here, HEAD_DIM)
    scaled = scaled.reshape(count, heads_here * HEAD_DIM)
    return (scaled * jax.nn.silu(emission_preactivation.astype(jnp.float32))).astype(jnp.bfloat16)

def row_norm(stream, mlp_scaling_factor):
    streamf = stream.astype(jnp.float32)
    squares = lax.optimization_barrier(jnp.mean(streamf * streamf, axis=-1, keepdims=True))
    return (streamf * lax.rsqrt(squares + EPSILON) * mlp_scaling_factor).astype(jnp.bfloat16)

def reference(skip_stream_vector, probe_preactivation, retention_preactivation, content_vector, emission_preactivation, retention_slack, surge_rate, subspace_scaling_factor, emission_matrix, mlp_scaling_factor, switch_matrix, expansion_matrix, contraction_matrix):
    arranged_sources = admission_source_matrix(probe_preactivation, retention_preactivation, content_vector, retention_slack, surge_rate)
    block_list = tuple((split_blocks(item, HEADS) for item in arranged_sources))
    start_carry = (jnp.zeros((HEADS, HEAD_DIM, HEAD_DIM), jnp.float32), jnp.zeros((HEADS, HEAD_DIM), jnp.float32))
    _, (outputs, _) = lax.scan(block_step, start_carry, block_list)
    outputs = outputs.transpose(0, 2, 1, 3).reshape(TOKENS, HEADS, HEAD_DIM)
    mixed = head_output(outputs, subspace_scaling_factor, emission_preactivation)
    projected = jnp.dot(mixed, emission_matrix, preferred_element_type=jnp.float32)
    stream = (skip_stream_vector.astype(jnp.float32) + projected).astype(jnp.bfloat16)
    normed = row_norm(stream, mlp_scaling_factor)
    gate_proj = jnp.dot(normed, switch_matrix, preferred_element_type=jnp.float32)
    up_proj = jnp.dot(normed, expansion_matrix, preferred_element_type=jnp.float32)
    hidden = (jax.nn.silu(gate_proj) * up_proj).astype(jnp.bfloat16)
    slice_width = FF // N_TP
    summed = jnp.zeros((TOKENS, D), jnp.float32)
    for member in range(N_TP):
        lower = member * slice_width
        partial_sum = jnp.dot(hidden[:, lower:lower + slice_width], contraction_matrix[lower:lower + slice_width], preferred_element_type=jnp.float32)
        summed = summed + partial_sum.astype(jnp.bfloat16).astype(jnp.float32)
    return (stream.astype(jnp.float32) + summed).astype(jnp.bfloat16)
```

```python
import functools

import jax
import jax.numpy as jnp
from jax import lax
from jax.experimental import pallas as pl
from jax.experimental.pallas import tpu as pltpu
from jax.sharding import Mesh
from jax.sharding import PartitionSpec as P

HEAD_DIM = 128
BLOCK = 64
EPSILON = 1e-06
F32 = jnp.float32
BF16 = jnp.bfloat16
ANY = pl.BlockSpec(memory_space=pl.ANY)
VMEM = pl.BlockSpec(memory_space=pltpu.VMEM)


NN = (((1,), (0,)), ((), ()))
NT = (((1,), (1,)), ((), ()))
TN = (((0,), (0,)), ((), ()))


def dot(a, b, dims=NN):
    return lax.dot_general(a, b, dims, preferred_element_type=F32)


def parts(a):
    high = a.astype(BF16)
    return high, (a - high.astype(F32)).astype(BF16)


def dot_split(a, b, dims):
    a_high, a_low = parts(a)
    b_high, b_low = parts(b)
    return dot(a_high, b_high, dims) + (dot(a_high, b_low, dims) + dot(a_low, b_high, dims))


def scan_kernel(probe, retention, content, slack, surge, out, carried, message, state, offset):
    rows, width = probe.shape
    heads = width // HEAD_DIM
    state[...] = jnp.zeros_like(state)
    offset[...] = jnp.zeros_like(offset)
    first = lax.broadcasted_iota(jnp.int32, (BLOCK, BLOCK), 0)
    second = lax.broadcasted_iota(jnp.int32, (BLOCK, BLOCK), 1)
    causal = first >= second
    ones = jnp.where(causal, 1.0, 0.0).astype(BF16)

    def step(turn, _):
        here = pl.ds(pl.multiple_of(turn * BLOCK, BLOCK), BLOCK)
        before = probe[here, :].astype(F32)
        query = before * jax.nn.sigmoid(before)
        gate = slack[...] * jax.nn.sigmoid(-retention[here, :].astype(F32))
        rate = jnp.log1p(-gate) + surge[here, :]
        value = content[here, :]
        high = rate.astype(BF16)
        rest = rate - high.astype(F32)
        middle_part = rest.astype(BF16)
        low = (rest - middle_part.astype(F32)).astype(BF16)
        cumulative = dot(ones, high) + (dot(ones, middle_part) + dot(ones, low))
        middle = cumulative[BLOCK // 2 : BLOCK // 2 + 1, :]
        total = cumulative[BLOCK - 1 : BLOCK, :]
        left = query * jnp.exp(cumulative - middle)
        right = gate * jnp.exp(middle - cumulative)
        entering = query * jnp.exp(cumulative)
        leaving = gate * jnp.exp(total - cumulative)
        carried[here, :] = query * jnp.exp(cumulative + offset[...])
        decay = jnp.exp(total)
        for head in range(heads):
            lanes = slice(head * HEAD_DIM, (head + 1) * HEAD_DIM)
            scores = jnp.where(causal, dot_split(left[:, lanes], right[:, lanes], NT), 0.0)
            score_high, score_low = parts(scores)
            held = state[lanes, :]
            values = value[:, lanes]
            out[here, lanes] = dot_split(entering[:, lanes], held, NT) + (
                dot(score_high, values) + dot(score_low, values)
            )
            leave_high, leave_low = parts(leaving[:, lanes])
            state[lanes, :] = decay[:, lanes] * held + (
                dot(values, leave_high, TN) + dot(values, leave_low, TN)
            )
        offset[...] += total
        return 0

    lax.fori_loop(0, rows // BLOCK, step, 0)
    message[0:width, :] = state[...].astype(BF16)
    final = jnp.exp(offset[...])
    tail = jnp.concatenate(
        [final[:, h * HEAD_DIM : (h + 1) * HEAD_DIM] for h in range(heads)]
        + [jnp.zeros((16 - heads, HEAD_DIM), F32)],
        axis=0,
    )
    message[width : width + 16, :] = tail.astype(BF16)


def local_scan(probe, retention, content, slack, surge):
    rows, width = probe.shape
    return pl.pallas_call(
        scan_kernel,
        out_shape=(
            jax.ShapeDtypeStruct((rows, width), F32),
            jax.ShapeDtypeStruct((rows, width), F32),
            jax.ShapeDtypeStruct((width + 16, HEAD_DIM), BF16),
        ),
        in_specs=[VMEM] * 5,
        out_specs=(VMEM, VMEM, VMEM),
        scratch_shapes=[pltpu.VMEM((width, HEAD_DIM), F32), pltpu.VMEM((1, width), F32)],
        name="local_scan",
    )(probe, retention, content, slack.reshape(1, width), surge)


def mix_kernel(out, carried, state, emission, gain, mixed):
    for head in range(out.shape[1] // HEAD_DIM):
        lanes = slice(head * HEAD_DIM, (head + 1) * HEAD_DIM)
        whole = out[:, lanes] + dot_split(carried[:, lanes], state[lanes, :], NT)
        squares = jnp.mean(whole * whole, axis=-1, keepdims=True)
        before = emission[:, lanes].astype(F32)
        scaled = whole * lax.rsqrt(squares + EPSILON) * gain[:, lanes]
        mixed[:, lanes] = (scaled * (before * jax.nn.sigmoid(before))).astype(BF16)


def mix(out, carried, state, emission, gain):
    rows, width = out.shape
    tile = min(256, rows)
    row_spec = pl.BlockSpec((tile, width), lambda i: (i, 0))
    return pl.pallas_call(
        mix_kernel,
        grid=(rows // tile,),
        out_shape=jax.ShapeDtypeStruct((rows, width), BF16),
        in_specs=[
            row_spec,
            row_spec,
            pl.BlockSpec((width, HEAD_DIM), lambda i: (0, 0)),
            row_spec,
            pl.BlockSpec((1, width), lambda i: (0, 0)),
        ],
        out_specs=row_spec,
        name="mix",
    )(out, carried, state, emission, gain.reshape(1, width))


def project_kernel(count, order, *refs):
    mixed, (weight, skip, gain, stream, normed) = refs[:count], refs[count:]
    width = mixed[0].shape[1]
    total = None
    for index in range(count):
        rows = pl.ds(pl.multiple_of(order[index] * width, width), width)
        term = dot(mixed[index][...], weight[rows, :])
        total = term if total is None else total + term
    added = (skip[...].astype(F32) + total).astype(BF16)
    stream[...] = added
    wide = added.astype(F32)
    squares = jnp.mean(wide * wide, axis=-1, keepdims=True)
    normed[...] = (wide * lax.rsqrt(squares + EPSILON) * gain[...]).astype(BF16)


def project(mixed, order, weight, skip, gain):
    rows, width = mixed[0].shape
    features = weight.shape[1]
    count = len(mixed)
    tile = min(256, rows)
    wide = pl.BlockSpec((tile, features), lambda i, o: (i, 0))
    return pl.pallas_call(
        functools.partial(project_kernel, count),
        grid_spec=pltpu.PrefetchScalarGridSpec(
            num_scalar_prefetch=1,
            grid=(rows // tile,),
            in_specs=[pl.BlockSpec((tile, width), lambda i, o: (i, 0))] * count
            + [
                pl.BlockSpec(weight.shape, lambda i, o: (0, 0)),
                wide,
                pl.BlockSpec((1, features), lambda i, o: (0, 0)),
            ],
            out_specs=(wide, wide),
        ),
        out_shape=(
            jax.ShapeDtypeStruct((rows, features), BF16),
            jax.ShapeDtypeStruct((rows, features), BF16),
        ),
        name="project",
    )(order, *mixed, weight, skip, gain.reshape(1, features))


def picked(line, length, offset, lower, upper, act):
    if offset == 0:
        act(lower)
        return

    @pl.when(line >= offset)
    def _():
        act(lower)

    @pl.when(line < offset)
    def _():
        act(upper)


def hidden_kernel(length, *refs):
    blocks = 4 * (2 * length - 1)
    weights, (normed, hidden, gate_all, up_all, sems) = refs[:blocks], refs[blocks:]
    depth = weights[0].shape[0]
    line = lax.axis_index("so")
    core = lax.axis_index("ti")

    def each(act):
        for matrix in range(2):
            for twin in range(2):
                start = (2 * matrix + twin) * (2 * length - 1)
                mine = weights[start : start + 2 * length - 1]
                target = (gate_all, up_all)[matrix]
                for offset in range(length):
                    place = lax.rem(line - offset + length, length)
                    side = core if twin == 0 else 1 - core
                    row = pl.multiple_of((2 * place + side) * depth, depth)
                    slot = (matrix * 2 + twin) * length + offset
                    act(
                        mine[offset],
                        mine[length - 1 + offset] if offset else None,
                        offset,
                        target.at[pl.ds(row, depth), :],
                        sems.at[slot],
                    )

    @pl.when(pl.program_id(0) == 0)
    def _():
        each(
            lambda lower, upper, offset, target, sem: picked(
                line,
                length,
                offset,
                lower,
                upper,
                lambda source: pltpu.make_async_copy(source, target, sem).start(),
            )
        )
        each(
            lambda lower, upper, offset, target, sem: pltpu.make_async_copy(
                lower, target, sem
            ).wait()
        )

    gate = dot(normed[...], gate_all[...])
    up = dot(normed[...], up_all[...])
    hidden[...] = (gate * jax.nn.sigmoid(gate) * up).astype(BF16)


def make_hidden(normed, weights, length):
    rows, features = normed.shape
    units = weights[0].shape[1]
    tile = min(256, rows)
    return pl.pallas_call(
        functools.partial(hidden_kernel, length),
        grid=(rows // tile,),
        out_shape=jax.ShapeDtypeStruct((rows, units), BF16),
        in_specs=[ANY] * len(weights) + [pl.BlockSpec((tile, features), lambda i: (i, 0))],
        out_specs=pl.BlockSpec((tile, units), lambda i: (i, 0)),
        scratch_shapes=[
            pltpu.VMEM((features, units), BF16),
            pltpu.VMEM((features, units), BF16),
            pltpu.SemaphoreType.DMA((4 * length,)),
        ],
        compiler_params=pltpu.CompilerParams(vmem_limit_bytes=56 * 1024 * 1024),
        name="make_hidden",
    )(*weights, normed)


def down_kernel(offset, length, count, order, hidden, lower, lower_twin, *refs):
    if offset:
        upper, upper_twin = refs[:2]
        refs = refs[2:]
    else:
        upper = upper_twin = None
    outs, (weight, sems) = refs[:count], refs[count:]
    columns = lower.shape[1]
    line = lax.axis_index("so")
    for twin, (low, high) in enumerate(((lower, upper), (lower_twin, upper_twin))):
        target = weight.at[:, pl.ds(twin * columns, columns)]
        picked(
            line,
            length,
            offset,
            low,
            high,
            lambda source: pltpu.make_async_copy(source, target, sems.at[twin]).start(),
        )
    for twin, low in enumerate((lower, lower_twin)):
        target = weight.at[:, pl.ds(twin * columns, columns)]
        pltpu.make_async_copy(low, target, sems.at[twin]).wait()
    rows = outs[0].shape[0]
    for index in range(count):
        here = pl.ds(pl.multiple_of(order[index] * rows, rows), rows)
        outs[index][...] = dot(hidden[here, :], weight[...]).astype(BF16)


def down(hidden, order, blocks, offset, length):
    rows, units = hidden.shape
    count = order.shape[0]
    columns = blocks[0].shape[1]
    shape = (rows // count, 2 * columns)
    return pl.pallas_call(
        functools.partial(down_kernel, offset, length, count),
        out_shape=[jax.ShapeDtypeStruct(shape, BF16)] * count,
        in_specs=[pl.BlockSpec(memory_space=pltpu.SMEM), VMEM] + [ANY] * len(blocks),
        out_specs=[VMEM] * count,
        scratch_shapes=[
            pltpu.VMEM((units, 2 * columns), BF16),
            pltpu.SemaphoreType.DMA((2,)),
        ],
        name="down",
    )(order, hidden, *blocks)


def finish_kernel(length, count, stream, *refs):
    pieces, out = refs[:-1], refs[-1]
    columns = pieces[0].shape[1] // 2
    line = lax.axis_index("so")
    side = lax.axis_index("si")
    for offset in range(length):
        place = lax.rem(line - offset + length, length)
        mine = pieces[offset * count : (offset + 1) * count]
        for twin in range(2):
            block = 2 * place + (side if twin == 0 else 1 - side)
            lanes = pl.ds(pl.multiple_of(block * columns, columns), columns)
            local = slice(twin * columns, (twin + 1) * columns)
            total = mine[0][:, local].astype(F32)
            for piece in mine[1:]:
                total = total + piece[:, local].astype(F32)
            out[:, lanes] = (stream[:, lanes].astype(F32) + total).astype(BF16)


def finish(stream, pieces, length, count):
    return pl.pallas_call(
        functools.partial(finish_kernel, length, count),
        out_shape=jax.ShapeDtypeStruct(stream.shape, BF16),
        in_specs=[VMEM] * (1 + len(pieces)),
        out_specs=VMEM,
        name="finish",
    )(stream, *pieces)


def on_device(
    length,
    ring,
    skip_stream_vector,
    probe_preactivation,
    retention_preactivation,
    content_vector,
    emission_preactivation,
    retention_slack,
    surge_rate,
    subspace_scaling_factor,
    emission_matrix,
    mlp_scaling_factor,
    switch_matrix,
    expansion_matrix,
    contraction_matrix,
):
    width = probe_preactivation.shape[1]
    heads = width // HEAD_DIM
    line = lax.axis_index("so")
    side = lax.axis_index("si")
    cross = lax.axis_index("to")
    core = lax.axis_index("ti")
    shifts = [(dx, dy) for dx in range(ring) for dy in range(2)]

    def swapped(a):
        return lax.ppermute(
            a, ("si", "ti"), [(2 * y + c, 2 * c + y) for y in range(2) for c in range(2)]
        )

    def traded(a, dx, dy):
        pairs = [
            ((y * ring + x) * 2 + c, ((c ^ dy) * ring + (x + dx) % ring) * 2 + y)
            for y in range(2)
            for x in range(ring)
            for c in range(2)
        ]
        return lax.ppermute(a, ("si", "to", "ti"), pairs)

    def returned(a, dx, dy):
        pairs = [
            ((y * ring + x) * 2 + c, (c * ring + (x + dx) % ring) * 2 + (y ^ dy))
            for y in range(2)
            for x in range(ring)
            for c in range(2)
        ]
        return lax.ppermute(a, ("si", "to", "ti"), pairs)

    def twin(a, places):
        pairs = [(2 * z + c, 2 * z + 1 - c) for z in places for c in range(2)]
        return lax.ppermute(a, ("so", "ti"), pairs)

    def spread(a):
        lower, upper = [a], [a]
        for k in range(1, length):
            lower.append(
                lax.ppermute(lower[-1], "so", [(i, i + 1) for i in range(k - 1, length - 1)])
            )
            upper.append(
                lax.ppermute(upper[-1], "so", [(i + 1, i) for i in range(0, length - k)])
            )
        mine = lower + upper[:0:-1]
        places = [range(k, length) for k in range(length)]
        places += [range(0, length - k) for k in range(length - 1, 0, -1)]
        return mine, [twin(block, place) for block, place in zip(mine, places)]

    gates, gate_twins = spread(swapped(switch_matrix))
    ups, up_twins = spread(swapped(expansion_matrix))
    downs, down_twins = spread(swapped(contraction_matrix))
    skips = [traded(skip_stream_vector, dx, dy) for dx, dy in shifts]

    out, carried, message = local_scan(
        probe_preactivation, retention_preactivation, content_vector, retention_slack, surge_rate
    )

    def opened(a):
        a = a.astype(F32)
        return a[:width].reshape(heads, HEAD_DIM, HEAD_DIM), a[width : width + heads][:, None, :]

    def closed(state, decay):
        return jnp.concatenate(
            [
                state.reshape(width, HEAD_DIM),
                decay.reshape(heads, HEAD_DIM),
                jnp.zeros((16 - heads, HEAD_DIM), F32),
            ]
        ).astype(BF16)

    other = lax.ppermute(message, "si", [(0, 1), (1, 0)])
    first_state, first_decay = opened(jnp.where(side == 0, message, other))
    second_state, second_decay = opened(jnp.where(side == 0, other, message))
    plane = closed(second_decay * first_state + second_state, first_decay * second_decay)
    incoming = jnp.zeros_like(first_state)
    weight = jnp.ones_like(first_decay)
    for k in range(1, length):
        state, decay = opened(
            lax.ppermute(plane, "so", [(i, i + k) for i in range(length - k)])
        )
        incoming = incoming + weight * state
        weight = weight * decay
    incoming = jnp.where(side == 0, incoming, first_decay * incoming + first_state)
    mixed = mix(
        out,
        carried,
        incoming.reshape(width, HEAD_DIM),
        emission_preactivation,
        subspace_scaling_factor,
    )

    mixed_blocks = [traded(mixed, dx, dy) for dx, dy in shifts]
    came = [lax.rem(cross - dx + ring, ring) * 2 + (side ^ dy) for dx, dy in shifts]
    goes = [lax.rem(cross + dx, ring) * 2 + (side ^ dy) for dx, dy in shifts]
    own_rows = skip_stream_vector.shape[0]
    skip_all = jnp.zeros((own_rows * len(shifts), skip_stream_vector.shape[1]), BF16)
    for rows, place in zip(skips, came):
        skip_all = lax.dynamic_update_slice_in_dim(skip_all, rows, place * own_rows, 0)
    stream, normed = project(
        mixed_blocks,
        jnp.stack(came).astype(jnp.int32),
        emission_matrix,
        skip_all,
        mlp_scaling_factor,
    )
    hidden = make_hidden(normed, gates + gate_twins + ups + up_twins, length)

    kept = lax.dynamic_slice_in_dim(stream, (2 * cross + core) * own_rows, own_rows, 0)
    given = lax.dynamic_slice_in_dim(stream, (2 * cross + 1 - core) * own_rows, own_rows, 0)
    own_stream = jnp.where(side == core, kept, twin(given, range(length)))

    order = jnp.stack(goes).astype(jnp.int32)
    pieces = []
    for offset in range(length):
        blocks = [downs[offset], down_twins[offset]]
        if offset:
            blocks += [downs[length - 1 + offset], down_twins[length - 1 + offset]]
        for part, (dx, dy) in zip(down(hidden, order, blocks, offset, length), shifts):
            pieces.append(returned(part, dx, dy))
    return finish(own_stream, pieces, length, len(shifts))


def solution(mesh):
    length, ring = mesh.shape["sp"] // 2, mesh.shape["tp"] // 2
    split = Mesh(mesh.devices.reshape(length, 2, ring, 2), ("so", "si", "to", "ti"))
    sp, tp = ("so", "si"), ("to", "ti")
    in_specs = (
        P(sp + tp, None),
        P(sp, tp),
        P(sp, tp),
        P(sp, tp),
        P(sp, tp),
        P(tp),
        P(sp, tp),
        P(tp),
        P(),
        P(),
        P(sp, tp),
        P(sp, tp),
        P(tp, sp),
    )
    return jax.shard_map(
        functools.partial(on_device, length, ring),
        mesh=split,
        in_specs=in_specs,
        out_specs=P(sp + tp, None),
        check_vma=False,
    )
```

```python
import functools

import jax
import jax.numpy as jnp
from jax import lax
from jax.experimental import pallas as pl
from jax.experimental.pallas import tpu as pltpu
from jax.sharding import Mesh
from jax.sharding import PartitionSpec as P


HEAD_DIM = 128
BLOCK = 64
CHUNK = 512
EPSILON = 1e-06
F32 = jnp.float32
BF16 = jnp.bfloat16
ANY = pl.BlockSpec(memory_space=pltpu.HBM)
VMEM = pl.BlockSpec(memory_space=pltpu.VMEM)


NN = (((1,), (0,)), ((), ()))
NT = (((1,), (1,)), ((), ()))
TN = (((0,), (0,)), ((), ()))


def dot(a, b, dims=NN):
    return lax.dot_general(a, b, dims, preferred_element_type=F32)


def parts(a):
    high = a.astype(BF16)
    return high, (a - high.astype(F32)).astype(BF16)


def dot_split(a, b, dims):
    a_high, a_low = parts(a)
    b_high, b_low = parts(b)
    return dot(a_high, b_high, dims) + (dot(a_high, b_low, dims) + dot(a_low, b_high, dims))


def scan_kernel(probe, retention, content, slack, surge, out, carried, message, state, offset):
    rows, width = probe.shape
    heads = width // HEAD_DIM
    state[...] = jnp.zeros_like(state)
    offset[...] = jnp.zeros_like(offset)
    first = lax.broadcasted_iota(jnp.int32, (BLOCK, BLOCK), 0)
    second = lax.broadcasted_iota(jnp.int32, (BLOCK, BLOCK), 1)
    causal = first >= second
    ones = jnp.where(causal, 1.0, 0.0).astype(BF16)

    def step(turn, _):
        here = pl.ds(pl.multiple_of(turn * BLOCK, BLOCK), BLOCK)
        before = probe[here, :].astype(F32)
        query = before * jax.nn.sigmoid(before)
        gate = slack[...] * jax.nn.sigmoid(-retention[here, :].astype(F32))
        rate = jnp.log1p(-gate) + surge[here, :]
        value = content[here, :]
        high = rate.astype(BF16)
        rest = rate - high.astype(F32)
        middle_part = rest.astype(BF16)
        low = (rest - middle_part.astype(F32)).astype(BF16)
        cumulative = dot(ones, high) + (dot(ones, middle_part) + dot(ones, low))
        middle = cumulative[BLOCK // 2 : BLOCK // 2 + 1, :]
        total = cumulative[BLOCK - 1 : BLOCK, :]
        left = query * jnp.exp(cumulative - middle)
        right = gate * jnp.exp(middle - cumulative)
        entering = query * jnp.exp(cumulative)
        leaving = gate * jnp.exp(total - cumulative)
        carried[here, :] = query * jnp.exp(cumulative + offset[...])
        decay = jnp.exp(total)
        for head in range(heads):
            lanes = slice(head * HEAD_DIM, (head + 1) * HEAD_DIM)
            scores = jnp.where(causal, dot_split(left[:, lanes], right[:, lanes], NT), 0.0)
            score_high, score_low = parts(scores)
            held = state[lanes, :]
            values = value[:, lanes]
            out[here, lanes] = dot_split(entering[:, lanes], held, NT) + (
                dot(score_high, values) + dot(score_low, values)
            )
            leave_high, leave_low = parts(leaving[:, lanes])
            state[lanes, :] = decay[:, lanes] * held + (
                dot(values, leave_high, TN) + dot(values, leave_low, TN)
            )
        offset[...] += total
        return 0

    lax.fori_loop(0, rows // BLOCK, step, 0, unroll=2)
    message[0:width, :] = state[...].astype(BF16)
    final = jnp.exp(offset[...])
    tail = jnp.concatenate(
        [final[:, h * HEAD_DIM : (h + 1) * HEAD_DIM] for h in range(heads)]
        + [jnp.zeros((16 - heads, HEAD_DIM), F32)],
        axis=0,
    )
    message[width : width + 16, :] = tail.astype(BF16)


def local_scan(probe, retention, content, slack, surge):
    rows, width = probe.shape
    return pl.pallas_call(
        scan_kernel,
        out_shape=(
            jax.ShapeDtypeStruct((rows, width), F32),
            jax.ShapeDtypeStruct((rows, width), F32),
            jax.ShapeDtypeStruct((width + 16, HEAD_DIM), BF16),
        ),
        in_specs=[VMEM] * 5,
        out_specs=(VMEM, VMEM, VMEM),
        scratch_shapes=[pltpu.VMEM((width, HEAD_DIM), F32), pltpu.VMEM((1, width), F32)],
        name="local_scan",
    )(probe, retention, content, slack.reshape(1, width), surge)


def mix_kernel(order, out, carried, state, emission, gain, *pieces):
    for head in range(out.shape[1] // HEAD_DIM):
        lanes = slice(head * HEAD_DIM, (head + 1) * HEAD_DIM)
        whole = out[:, lanes] + dot_split(carried[:, lanes], state[lanes, :], NT)
        squares = jnp.mean(whole * whole, axis=-1, keepdims=True)
        before = emission[:, lanes].astype(F32)
        scaled = whole * lax.rsqrt(squares + EPSILON) * gain[:, lanes]
        mixed = (scaled * (before * jax.nn.sigmoid(before))).astype(BF16)
        for index, piece in enumerate(pieces):

            @pl.when(pl.program_id(0) == index)
            def _(piece=piece):
                piece[:, lanes] = mixed


def mix(out, carried, state, emission, gain, order):
    rows, width = out.shape
    count = order.shape[0]
    tile = rows // count
    row_spec = pl.BlockSpec((tile, width), lambda i, o: (o[i], 0))
    return pl.pallas_call(
        mix_kernel,
        grid_spec=pltpu.PrefetchScalarGridSpec(
            num_scalar_prefetch=1,
            grid=(count,),
            in_specs=[
                row_spec,
                row_spec,
                pl.BlockSpec((width, HEAD_DIM), lambda i, o: (0, 0)),
                row_spec,
                pl.BlockSpec((1, width), lambda i, o: (0, 0)),
            ],
            out_specs=[pl.BlockSpec((tile, width), lambda i, o: (0, 0))] * count,
        ),
        out_shape=[jax.ShapeDtypeStruct((tile, width), BF16)] * count,
        name="mix",
    )(order, out, carried, state, emission, gain.reshape(1, width))


def project_kernel(count, order, *refs):
    mixed, (weight, skip, gain, stream, normed) = refs[:count], refs[count:]
    width = mixed[0].shape[1]
    total = None
    for index in range(count):
        rows = pl.ds(pl.multiple_of(order[index] * width, width), width)
        term = dot(mixed[index][...], weight[rows, :])
        total = term if total is None else total + term
    added = (skip[...].astype(F32) + total).astype(BF16)
    stream[...] = added
    wide = added.astype(F32)
    squares = jnp.mean(wide * wide, axis=-1, keepdims=True)
    normed[...] = (wide * lax.rsqrt(squares + EPSILON) * gain[...]).astype(BF16)


def project(mixed, order, weight, skip, gain):
    count = len(mixed)
    shape = jax.ShapeDtypeStruct(skip.shape, BF16)
    return pl.pallas_call(
        functools.partial(project_kernel, count),
        in_specs=[pl.BlockSpec(memory_space=pltpu.SMEM)] + [VMEM] * (count + 3),
        out_specs=(VMEM, VMEM),
        out_shape=(shape, shape),
        name="project",
    )(order, *mixed, weight, skip, gain.reshape(1, -1))


def arrivals(length, line):
    below = [(steps, 0) for steps in range(1, line + 1)]
    above = [(steps, 1) for steps in range(1, length - line)]
    return [(0, 0)] + sorted(below + above)


def place_of(length, line, slot):
    result = 0
    for here in range(length):
        steps, side = arrivals(length, here)[slot]
        result = jnp.where(line == here, here + steps if side else here - steps, result)
    return result


def sources(length, slots):
    return [sorted({arrivals(length, here)[slot] for here in range(length)}) for slot in slots]


def pack_kernel(length, slots, matrices, *refs):
    line = lax.axis_index("so")
    packed, sems = refs[-2:]
    names = sources(length, slots)
    cursor = 0
    waits = []
    for matrix in range(matrices):
        for index, slot in enumerate(slots):
            target = packed.at[matrix * len(slots) + index]
            sem = sems.at[matrix * len(slots) + index]
            for name in names[index]:
                source = refs[cursor]
                cursor += 1
                chosen = functools.reduce(
                    jnp.logical_or,
                    [line == i for i in range(length) if arrivals(length, i)[slot] == name],
                )

                @pl.when(chosen)
                def _(source=source, target=target, sem=sem):
                    pltpu.make_async_copy(source, target, sem).start()

            waits.append((source, target, sem))
    for source, target, sem in waits:
        pltpu.make_async_copy(source, target, sem).wait()


def pack(chains, slots, length):
    blocks = [
        chain[name] for chain in chains for names in sources(length, slots) for name in names
    ]
    count = len(chains) * len(slots)
    return pl.pallas_call(
        functools.partial(pack_kernel, length, slots, len(chains)),
        out_shape=jax.ShapeDtypeStruct((count,) + blocks[0].shape, BF16),
        in_specs=[ANY] * len(blocks),
        out_specs=VMEM,
        scratch_shapes=[pltpu.SemaphoreType.DMA((count,))],
        name="pack",
    )(*blocks)


def hidden_kernel(length, groups, count, *refs):
    normed, refs = refs[:count], refs[count:]
    mine, twins = refs[: len(groups)], refs[len(groups) : 2 * len(groups)]
    hidden, rows_now, gate_all, up_all, sems = refs[2 * len(groups) :]
    depth = mine[0].shape[1]
    line = lax.axis_index("so")
    core = lax.axis_index("ti")

    @pl.when(pl.program_id(0) == 0)
    def _():
        copies = []
        for twin, packs in enumerate((mine, twins)):
            side = 1 - core if twin else core
            for pack_ref, slots in zip(packs, groups):
                for matrix, target in enumerate((gate_all, up_all)):
                    for index, slot in enumerate(slots):
                        row = (2 * place_of(length, line, slot) + side) * depth
                        copies.append(
                            pltpu.make_async_copy(
                                pack_ref.at[matrix * len(slots) + index],
                                target.at[pl.ds(pl.multiple_of(row, depth), depth), :],
                                sems.at[(2 * twin + matrix) * length + slot],
                            )
                        )
        for copy in copies:
            copy.start()
        for copy in copies:
            copy.wait()

    for index, piece in enumerate(normed):

        @pl.when(pl.program_id(0) == index)
        def _(piece=piece):
            rows_now[...] = piece[...]

    units = hidden.shape[2]
    for start in range(0, units, CHUNK):
        lanes = slice(start, min(start + CHUNK, units))
        gate = dot(rows_now[...], gate_all[:, lanes])
        up = dot(rows_now[...], up_all[:, lanes])
        hidden[0, :, lanes] = (gate * jax.nn.sigmoid(gate) * up).astype(BF16)


def make_hidden(normed, mine, twins, groups, length):
    rows, features = normed[0].shape
    units = mine[0].shape[2]
    count = len(normed)
    return pl.pallas_call(
        functools.partial(hidden_kernel, length, groups, count),
        grid=(count,),
        out_shape=jax.ShapeDtypeStruct((count, rows, units), BF16),
        in_specs=[pl.BlockSpec((rows, features), lambda i: (0, 0))] * count
        + [ANY] * (2 * len(groups)),
        out_specs=pl.BlockSpec((1, rows, units), lambda i: (i, 0, 0)),
        scratch_shapes=[
            pltpu.VMEM((rows, features), BF16),
            pltpu.VMEM((features, units), BF16),
            pltpu.VMEM((features, units), BF16),
            pltpu.SemaphoreType.DMA((4 * length,)),
        ],
        compiler_params=pltpu.CompilerParams(vmem_limit_bytes=56 * 1024 * 1024),
        name="make_hidden",
    )(*normed, *mine, *twins)


def down_kernel(count, hidden, mine, twins, *refs):
    outs, (weight, sems) = refs[:count], refs[count:]
    slots, columns = mine.shape[0], mine.shape[2]
    copies = []
    for twin, blocks in enumerate((mine, twins)):
        for slot in range(slots):
            target = weight.at[:, pl.ds((2 * slot + twin) * columns, columns)]
            copies.append(
                pltpu.make_async_copy(blocks.at[slot], target, sems.at[2 * slot + twin])
            )
    for copy in copies:
        copy.start()
    for copy in copies:
        copy.wait()
    for index in range(count):
        outs[index][...] = dot(hidden[index], weight[...]).astype(BF16)


def down(hidden, mine, twins):
    count, rows, units = hidden.shape
    width = 2 * mine.shape[0] * mine.shape[2]
    return pl.pallas_call(
        functools.partial(down_kernel, count),
        out_shape=[jax.ShapeDtypeStruct((rows, width), BF16)] * count,
        in_specs=[VMEM, ANY, ANY],
        out_specs=[VMEM] * count,
        scratch_shapes=[
            pltpu.VMEM((units, width), BF16),
            pltpu.SemaphoreType.DMA((2 * mine.shape[0],)),
        ],
        name="down",
    )(hidden, mine, twins)


def finish_kernel(length, groups, count, stream, *refs):
    pieces, out = refs[:-1], refs[-1]
    columns = stream.shape[1] // (2 * length)
    line = lax.axis_index("so")
    side = lax.axis_index("si")
    for group, slots in enumerate(groups):
        mine = pieces[group * count : (group + 1) * count]
        for index, slot in enumerate(slots):
            for twin in range(2):
                block = 2 * place_of(length, line, slot) + (1 - side if twin else side)
                lanes = pl.ds(pl.multiple_of(block * columns, columns), columns)
                start = (2 * index + twin) * columns
                local = slice(start, start + columns)
                total = mine[0][:, local].astype(F32)
                for piece in mine[1:]:
                    total = total + piece[:, local].astype(F32)
                out[:, lanes] = (stream[:, lanes].astype(F32) + total).astype(BF16)


def finish(stream, pieces, groups, length, count):
    return pl.pallas_call(
        functools.partial(finish_kernel, length, groups, count),
        out_shape=jax.ShapeDtypeStruct(stream.shape, BF16),
        in_specs=[VMEM] * (1 + len(pieces)),
        out_specs=VMEM,
        name="finish",
    )(stream, *pieces)


def on_device(
    length,
    ring,
    skip_stream_vector,
    probe_preactivation,
    retention_preactivation,
    content_vector,
    emission_preactivation,
    retention_slack,
    surge_rate,
    subspace_scaling_factor,
    emission_matrix,
    mlp_scaling_factor,
    switch_matrix,
    expansion_matrix,
    contraction_matrix,
):
    width = probe_preactivation.shape[1]
    heads = width // HEAD_DIM
    side = lax.axis_index("si")
    cross = lax.axis_index("to")
    core = lax.axis_index("ti")
    shifts = [(dx, dy) for dx in range(ring) for dy in range(2)]
    up_groups, down_groups = groups_of(length)

    def swapped(a):
        pairs = [(2 * y + c, 2 * c + y) for y in range(2) for c in range(2)]
        return lax.ppermute(a, ("si", "ti"), pairs)

    def traded(a, dx, dy):
        pairs = [
            ((y * ring + x) * 2 + c, ((c ^ dy) * ring + (x + dx) % ring) * 2 + y)
            for y in range(2)
            for x in range(ring)
            for c in range(2)
        ]
        return lax.ppermute(a, ("si", "to", "ti"), pairs)

    def returned(a, dx, dy):
        pairs = [
            (((c ^ dy) * ring + (x + dx) % ring) * 2 + y, (y * ring + x) * 2 + c)
            for y in range(2)
            for x in range(ring)
            for c in range(2)
        ]
        return lax.ppermute(a, ("si", "to", "ti"), pairs)

    def dealt(a, dx, dc):
        pairs = [
            (2 * x + c, 2 * ((x + dx) % ring) + (c ^ dc)) for x in range(ring) for c in range(2)
        ]
        return lax.ppermute(a, ("to", "ti"), pairs)

    def twin(a):
        return lax.ppermute(a, "ti", [(0, 1), (1, 0)])

    def spread(a, direct=False):
        chain = {(0, 0): a}
        lower = upper = a
        for k in range(1, length):
            hop = k if direct else 1
            source = (a, a) if direct else (lower, upper)
            pairs = [(i, i + hop) for i in range(k - hop, length - hop)]
            lower = chain[k, 0] = lax.ppermute(source[0], "so", pairs)
            pairs = [(i + hop, i) for i in range(0, length - k)]
            upper = chain[k, 1] = lax.ppermute(source[1], "so", pairs)
        return chain

    gates = spread(swapped(switch_matrix))
    ups = spread(swapped(expansion_matrix))
    downs = spread(swapped(contraction_matrix), direct=True)

    out, carried, message = local_scan(
        probe_preactivation,
        retention_preactivation,
        content_vector,
        retention_slack,
        surge_rate,
    )

    def opened(a):
        a = a.astype(F32)
        return a[:width].reshape(heads, HEAD_DIM, HEAD_DIM), a[width : width + heads][:, None, :]

    def closed(state, decay):
        return jnp.concatenate(
            [
                state.reshape(width, HEAD_DIM),
                decay.reshape(heads, HEAD_DIM),
                jnp.zeros((16 - heads, HEAD_DIM), F32),
            ]
        ).astype(BF16)

    other = lax.ppermute(message, "si", [(0, 1), (1, 0)])
    first_state, first_decay = opened(jnp.where(side == 0, message, other))
    second_state, second_decay = opened(jnp.where(side == 0, other, message))
    plane = closed(second_decay * first_state + second_state, first_decay * second_decay)
    incoming = jnp.zeros_like(first_state)
    weight = jnp.ones_like(first_decay)
    for k in range(1, length):
        pairs = [(i, i + k) for i in range(length - k)]
        state, decay = opened(lax.ppermute(plane, "so", pairs))
        incoming = incoming + weight * state
        weight = weight * decay
    incoming = jnp.where(side == 0, incoming, first_decay * incoming + first_state)
    came = [lax.rem(cross - dx + ring, ring) * 2 + (core ^ dc) for dx, dc in shifts]
    goes = [lax.rem(cross + dx, ring) * 2 + (core ^ dc) for dx, dc in shifts]
    mixed = mix(
        out,
        carried,
        incoming.reshape(width, HEAD_DIM),
        emission_preactivation,
        subspace_scaling_factor,
        jnp.stack(goes).astype(jnp.int32),
    )
    mixed = [mixed[0]] + [dealt(mixed[index], *shifts[index]) for index in range(1, len(shifts))]
    stream, normed = project(
        mixed,
        jnp.stack(came).astype(jnp.int32),
        emission_matrix,
        skip_stream_vector,
        mlp_scaling_factor,
    )
    normed = [traded(normed, dx, dy) for dx, dy in shifts]

    packs, pack_twins = [], []
    for slots in up_groups:
        packs.append(pack((gates, ups), slots, length))
        pack_twins.append(twin(packs[-1]))
    hidden = make_hidden(normed, packs, pack_twins, up_groups, length)

    pieces = []
    for slots in down_groups:
        mine = pack((downs,), slots, length)
        both = twin(mine)
        parts_out = down(hidden, mine, both)
        for index, (dx, dy) in enumerate(shifts):
            pieces.append(returned(parts_out[index], dx, dy))
    return finish(stream, pieces, down_groups, length, len(shifts))


def groups_of(length):
    last = length - 1
    return (
        (tuple(range(last)), (last,)),
        (tuple(range(last - 1)), (last - 1, last)),
    )


def solution(mesh):
    length, ring = mesh.shape["sp"] // 2, mesh.shape["tp"] // 2
    split = Mesh(mesh.devices.reshape(length, 2, ring, 2), ("so", "si", "to", "ti"))
    sp, tp = ("so", "si"), ("to", "ti")
    in_specs = (
        P(sp + tp, None),
        P(sp, tp),
        P(sp, tp),
        P(sp, tp),
        P(sp, tp),
        P(tp),
        P(sp, tp),
        P(tp),
        P(),
        P(),
        P(sp, tp),
        P(sp, tp),
        P(tp, sp),
    )


    def body(*arguments):
        return on_device(length, ring, *arguments)

    return jax.shard_map(
        body, mesh=split, in_specs=in_specs, out_specs=P(sp + tp, None), check_vma=False
    )
```

```python
import functools

import jax
import jax.numpy as jnp
from jax import lax
from jax.experimental import pallas as pl
from jax.experimental.pallas import tpu as pltpu
from jax.sharding import Mesh
from jax.sharding import PartitionSpec as P


HEAD_DIM = 128
BLOCK = 64
CHUNK = 512
ROOM = 66_000_000
EPSILON = 1e-06
F32 = jnp.float32
BF16 = jnp.bfloat16
ANY = pl.BlockSpec(memory_space=pltpu.HBM)
VMEM = pl.BlockSpec(memory_space=pltpu.VMEM)


NN = (((1,), (0,)), ((), ()))
NT = (((1,), (1,)), ((), ()))
TN = (((0,), (0,)), ((), ()))


def dot(a, b, dims=NN):
    return lax.dot_general(a, b, dims, preferred_element_type=F32)


def parts(a):
    high = a.astype(BF16)
    return high, (a - high.astype(F32)).astype(BF16)


def dot_split(a, b, dims):
    a_high, a_low = parts(a)
    b_high, b_low = parts(b)
    return dot(a_high, b_high, dims) + (dot(a_high, b_low, dims) + dot(a_low, b_high, dims))


def scan_kernel(probe, retention, content, slack, surge, out, carried, message, state, offset):
    rows, width = probe.shape
    heads = width // HEAD_DIM
    state[...] = jnp.zeros_like(state)
    offset[...] = jnp.zeros_like(offset)
    first = lax.broadcasted_iota(jnp.int32, (BLOCK, BLOCK), 0)
    second = lax.broadcasted_iota(jnp.int32, (BLOCK, BLOCK), 1)
    causal = first >= second
    ones = jnp.where(causal, 1.0, 0.0).astype(BF16)

    def step(turn, _):
        here = pl.ds(pl.multiple_of(turn * BLOCK, BLOCK), BLOCK)
        before = probe[here, :].astype(F32)
        query = before * jax.nn.sigmoid(before)
        gate = slack[...] * jax.nn.sigmoid(-retention[here, :].astype(F32))
        rate = jnp.log1p(-gate) + surge[here, :]
        value = content[here, :]
        high = rate.astype(BF16)
        rest = rate - high.astype(F32)
        middle_part = rest.astype(BF16)
        low = (rest - middle_part.astype(F32)).astype(BF16)
        cumulative = dot(ones, high) + (dot(ones, middle_part) + dot(ones, low))
        middle = cumulative[BLOCK // 2 : BLOCK // 2 + 1, :]
        total = cumulative[BLOCK - 1 : BLOCK, :]
        left = query * jnp.exp(cumulative - middle)
        right = gate * jnp.exp(middle - cumulative)
        entering = query * jnp.exp(cumulative)
        leaving = gate * jnp.exp(total - cumulative)
        carried[here, :] = query * jnp.exp(cumulative + offset[...])
        decay = jnp.exp(total)
        for head in range(heads):
            lanes = slice(head * HEAD_DIM, (head + 1) * HEAD_DIM)
            scores = jnp.where(causal, dot_split(left[:, lanes], right[:, lanes], NT), 0.0)
            score_high, score_low = parts(scores)
            held = state[lanes, :]
            values = value[:, lanes]
            out[here, lanes] = dot_split(entering[:, lanes], held, NT) + (
                dot(score_high, values) + dot(score_low, values)
            )
            leave_high, leave_low = parts(leaving[:, lanes])
            state[lanes, :] = decay[:, lanes] * held + (
                dot(values, leave_high, TN) + dot(values, leave_low, TN)
            )
        offset[...] += total
        return 0

    lax.fori_loop(0, rows // BLOCK, step, 0, unroll=4)
    message[0:width, :] = state[...].astype(BF16)
    final = jnp.exp(offset[...])
    tail = jnp.concatenate(
        [final[:, h * HEAD_DIM : (h + 1) * HEAD_DIM] for h in range(heads)]
        + [jnp.zeros((16 - heads, HEAD_DIM), F32)],
        axis=0,
    )
    message[width : width + 16, :] = tail.astype(BF16)


def local_scan(probe, retention, content, slack, surge):
    rows, width = probe.shape
    return pl.pallas_call(
        scan_kernel,
        out_shape=(
            jax.ShapeDtypeStruct((rows, width), F32),
            jax.ShapeDtypeStruct((rows, width), F32),
            jax.ShapeDtypeStruct((width + 16, HEAD_DIM), BF16),
        ),
        in_specs=[VMEM] * 5,
        out_specs=(VMEM, VMEM, VMEM),
        scratch_shapes=[pltpu.VMEM((width, HEAD_DIM), F32), pltpu.VMEM((1, width), F32)],
        name="local_scan",
    )(probe, retention, content, slack.reshape(1, width), surge)


def mix_kernel(order, out, carried, state, emission, gain, *pieces):
    for head in range(out.shape[1] // HEAD_DIM):
        lanes = slice(head * HEAD_DIM, (head + 1) * HEAD_DIM)
        whole = out[:, lanes] + dot_split(carried[:, lanes], state[lanes, :], NT)
        squares = jnp.mean(whole * whole, axis=-1, keepdims=True)
        before = emission[:, lanes].astype(F32)
        scaled = whole * lax.rsqrt(squares + EPSILON) * gain[:, lanes]
        mixed = (scaled * (before * jax.nn.sigmoid(before))).astype(BF16)
        for index, piece in enumerate(pieces):

            @pl.when(pl.program_id(0) == index)
            def _(piece=piece):
                piece[:, lanes] = mixed


def mix(out, carried, state, emission, gain, order):
    rows, width = out.shape
    count = order.shape[0]
    tile = rows // count
    row_spec = pl.BlockSpec((tile, width), lambda i, o: (o[i], 0))
    return pl.pallas_call(
        mix_kernel,
        grid_spec=pltpu.PrefetchScalarGridSpec(
            num_scalar_prefetch=1,
            grid=(count,),
            in_specs=[
                row_spec,
                row_spec,
                pl.BlockSpec((width, HEAD_DIM), lambda i, o: (0, 0)),
                row_spec,
                pl.BlockSpec((1, width), lambda i, o: (0, 0)),
            ],
            out_specs=[pl.BlockSpec((tile, width), lambda i, o: (0, 0))] * count,
        ),
        out_shape=[jax.ShapeDtypeStruct((tile, width), BF16)] * count,
        name="mix",
    )(order, out, carried, state, emission, gain.reshape(1, width))


def project_kernel(count, order, *refs):
    mixed, (weight, skip, gain, stream, normed) = refs[:count], refs[count:]
    width = mixed[0].shape[1]
    total = None
    for index in range(count):
        rows = pl.ds(pl.multiple_of(order[index] * width, width), width)
        term = dot(mixed[index][...], weight[rows, :])
        total = term if total is None else total + term
    added = (skip[...].astype(F32) + total).astype(BF16)
    stream[...] = added
    wide = added.astype(F32)
    squares = jnp.mean(wide * wide, axis=-1, keepdims=True)
    normed[...] = (wide * lax.rsqrt(squares + EPSILON) * gain[...]).astype(BF16)


def project(mixed, order, weight, skip, gain):
    count = len(mixed)
    shape = jax.ShapeDtypeStruct(skip.shape, BF16)
    return pl.pallas_call(
        functools.partial(project_kernel, count),
        in_specs=[pl.BlockSpec(memory_space=pltpu.SMEM)] + [VMEM] * (count + 3),
        out_specs=(VMEM, VMEM),
        out_shape=(shape, shape),
        name="project",
    )(order, *mixed, weight, skip, gain.reshape(1, -1))


def arrivals(length):
    offsets = [0]
    for step in range(1, length // 2 + 1):
        offsets += [step, length - step][: min(2, length - len(offsets))]
    return offsets


def column_place(line, offset, length):
    return lax.rem(line - offset + length, length)


def pack_kernel(*refs):
    blocks, (packed, sems) = refs[:-2], refs[-2:]
    copies = [
        pltpu.make_async_copy(block, packed.at[index], sems.at[index])
        for index, block in enumerate(blocks)
    ]
    for copy in copies:
        copy.start()
    for copy in copies:
        copy.wait()


def pack(blocks):
    count = len(blocks)
    return pl.pallas_call(
        pack_kernel,
        out_shape=jax.ShapeDtypeStruct((count,) + blocks[0].shape, BF16),
        in_specs=[ANY] * count,
        out_specs=VMEM,
        scratch_shapes=[pltpu.SemaphoreType.DMA((count,))],
        name="pack",
    )(*blocks)


def hidden_kernel(length, count, *refs):
    normed, refs = refs[:count], refs[count:]
    gates, ups, refs = refs[:length], refs[length : 2 * length], refs[2 * length :]
    (packed, last_gate, last_up, down_own, down_twin), refs = refs[:5], refs[5:]
    hidden, outs, refs = refs[0], refs[1 : 1 + count], refs[1 + count :]
    rows_now, gate_all, up_all, down_all, gate_sum, up_sum, sems, piece_sem = refs
    depth, units = gates[0].shape
    columns = down_own.shape[1]
    line = lax.axis_index("so")
    core = lax.axis_index("ti")
    turn = pl.program_id(0)
    early = length - 1

    height = normed[0].shape[0]
    group = hidden.shape[0] // height
    half = length * depth

    places = []
    weight_copies = []
    for twin in range(2):
        side = 1 - core if twin else core
        for index, offset in enumerate(arrivals(length)):
            if not twin:
                gate_block, up_block = gates[index], ups[index]
            elif index < early:
                gate_block, up_block = packed.at[index], packed.at[early + index]
            else:
                gate_block, up_block = last_gate, last_up
            slot = twin * length + index
            rows = pl.ds(slot * depth, depth)
            weight_copies += [
                pltpu.make_async_copy(gate_block, gate_all.at[rows, :], sems.at[2 * slot]),
                pltpu.make_async_copy(up_block, up_all.at[rows, :], sems.at[2 * slot + 1]),
            ]
            places.append(2 * column_place(line, offset, length) + side)
    down_copies = [
        pltpu.make_async_copy(
            block, down_all.at[:, pl.ds(index * columns, columns)], sems.at[4 * length + index]
        )
        for index, block in enumerate((down_own, down_twin))
    ]

    def piece_copies(piece):
        return [
            pltpu.make_async_copy(
                normed[piece].at[:, pl.ds(pl.multiple_of(place * depth, depth), depth)],
                rows_now.at[pl.ds(piece * height, height), pl.ds(slot * depth, depth)],
                piece_sem.at[piece * 2 * length + slot],
            )
            for slot, place in enumerate(places)
        ]

    chunks = [slice(start, min(start + CHUNK, units)) for start in range(0, units, CHUNK)]

    @pl.when(turn == 0)
    def _():
        first = [copy for piece in range(group) for copy in piece_copies(piece)]
        others = [copy for piece in range(group, count) for copy in piece_copies(piece)]
        for copy in first + weight_copies + down_copies + others:
            copy.start()
        for copy in first + weight_copies[: 2 * length]:
            copy.wait()
        now = slice(0, group * height)
        for lanes in chunks:
            gate_sum[:, lanes] = dot(rows_now[now, :half], gate_all[:half, lanes])
            up_sum[:, lanes] = dot(rows_now[now, :half], up_all[:half, lanes])
        for copy in weight_copies[2 * length :]:
            copy.wait()
        for lanes in chunks:
            gate = gate_sum[:, lanes] + dot(rows_now[now, half:], gate_all[half:, lanes])
            up = up_sum[:, lanes] + dot(rows_now[now, half:], up_all[half:, lanes])
            hidden[:, lanes] = (gate * jax.nn.sigmoid(gate) * up).astype(BF16)
        for copy in down_copies:
            copy.wait()

    for piece in range(group, count):

        @pl.when(turn == piece // group)
        def _(piece=piece):
            for copy in piece_copies(piece):
                copy.wait()

    @pl.when(turn > 0)
    def _():
        here = pl.ds(pl.multiple_of(turn * group * height, group * height), group * height)
        for lanes in chunks:
            gate = dot(rows_now[here, :], gate_all[:, lanes])
            up = dot(rows_now[here, :], up_all[:, lanes])
            hidden[:, lanes] = (gate * jax.nn.sigmoid(gate) * up).astype(BF16)

    share = dot(hidden[...], down_all[...]).astype(BF16)
    for index in range(count):

        @pl.when(turn == index // group)
        def _(index=index):
            start = index % group * height
            outs[index][...] = share[start : start + height, :]


def make_hidden(normed, gates, ups, packed, last_gate, last_up, down_own, down_twin):
    rows, features = normed[0].shape
    length = len(gates)
    units = gates[0].shape[1]
    columns = 2 * down_own.shape[1]
    count = len(normed)
    return pl.pallas_call(
        functools.partial(hidden_kernel, length, count),
        grid=(count // 2,),
        out_shape=[jax.ShapeDtypeStruct((count * rows, units), BF16)]
        + [jax.ShapeDtypeStruct((rows, columns), BF16)] * count,
        in_specs=[ANY] * (count + 2 * length + 5),
        out_specs=[pl.BlockSpec((2 * rows, units), lambda i: (i, 0))]
        + [pl.BlockSpec((rows, columns), lambda i: (0, 0))] * count,
        scratch_shapes=[
            pltpu.VMEM((count * rows, features), BF16),
            pltpu.VMEM((features, units), BF16),
            pltpu.VMEM((features, units), BF16),
            pltpu.VMEM((units, columns), BF16),
            pltpu.VMEM((2 * rows, units), F32),
            pltpu.VMEM((2 * rows, units), F32),
            pltpu.SemaphoreType.DMA((4 * length + 2,)),
            pltpu.SemaphoreType.DMA((2 * length * count,)),
        ],
        compiler_params=pltpu.CompilerParams(vmem_limit_bytes=ROOM),
        name="make_hidden",
    )(*normed, *gates, *ups, packed, last_gate, last_up, down_own, down_twin)


def down_kernel(count, blocks, hidden, *refs):
    weights, outs, (weight, sems) = refs[:blocks], refs[blocks : blocks + count], refs[-2:]
    columns = weights[0].shape[1]
    rows = outs[0].shape[0]
    copies = [
        pltpu.make_async_copy(
            block, weight.at[:, pl.ds(index * columns, columns)], sems.at[index]
        )
        for index, block in enumerate(weights)
    ]
    for copy in copies:
        copy.start()
    for copy in copies:
        copy.wait()
    for index in range(count):
        here = hidden[index * rows : (index + 1) * rows, :]
        outs[index][...] = dot(here, weight[...]).astype(BF16)


def down(hidden, blocks, count):
    rows, units = hidden.shape
    width = len(blocks) * blocks[0].shape[1]
    return pl.pallas_call(
        functools.partial(down_kernel, count, len(blocks)),
        out_shape=[jax.ShapeDtypeStruct((rows // count, width), BF16)] * count,
        in_specs=[VMEM] + [ANY] * len(blocks),
        out_specs=[VMEM] * count,
        scratch_shapes=[
            pltpu.VMEM((units, width), BF16),
            pltpu.SemaphoreType.DMA((len(blocks),)),
        ],
        name="down",
    )(hidden, *blocks)


def finish_kernel(length, groups, count, stream, *refs):
    pieces, out = refs[:-1], refs[-1]
    columns = stream.shape[1] // (2 * length)
    line = lax.axis_index("so")
    side = lax.axis_index("si")
    for group, offsets in enumerate(groups):
        mine = pieces[group * count : (group + 1) * count]
        for index, offset in enumerate(offsets):
            for twin in range(2):
                place = column_place(line, offset, length)
                block = 2 * place + (1 - side if twin else side)
                lanes = pl.ds(pl.multiple_of(block * columns, columns), columns)
                start = (2 * index + twin) * columns
                local = slice(start, start + columns)
                total = mine[0][:, local].astype(F32)
                for piece in mine[1:]:
                    total = total + piece[:, local].astype(F32)
                out[:, lanes] = (stream[:, lanes].astype(F32) + total).astype(BF16)


def finish(stream, pieces, groups, length, count):
    def kernel(stream_ref, *refs):
        refs[-1][...] = stream_ref[...]
        finish_kernel(length, groups, count, stream_ref, *refs)

    return pl.pallas_call(
        kernel,
        out_shape=jax.ShapeDtypeStruct(stream.shape, BF16),
        in_specs=[VMEM] * (1 + len(pieces)),
        out_specs=VMEM,
        name="finish",
    )(stream, *pieces)


def last_kernel(length, offsets, stream, *refs):
    pieces, (out, held, done, read_sems, write_sems) = refs[:-5], refs[-5:]
    columns = held.shape[2]
    line = lax.axis_index("so")
    side = lax.axis_index("si")
    moves = []
    for index, offset in enumerate(offsets):
        for twin in range(2):
            block = 2 * column_place(line, offset, length) + (1 - side if twin else side)
            lanes = pl.ds(pl.multiple_of(block * columns, columns), columns)
            slot = 2 * index + twin
            moves.append(
                (
                    pltpu.make_async_copy(stream.at[:, lanes], held.at[slot], read_sems.at[slot]),
                    pltpu.make_async_copy(done.at[slot], out.at[:, lanes], write_sems.at[slot]),
                )
            )
    for read, _ in moves:
        read.start()
    for slot, (read, write) in enumerate(moves):
        local = slice(slot * columns, (slot + 1) * columns)
        total = pieces[0][:, local].astype(F32)
        for piece in pieces[1:]:
            total = total + piece[:, local].astype(F32)
        read.wait()
        done[slot] = (held[slot].astype(F32) + total).astype(BF16)
        write.start()
    for _, write in moves:
        write.wait()


def finish_last(stream, pieces, offsets, length):
    rows = stream.shape[0]
    count = 2 * len(offsets)
    columns = pieces[0].shape[1] // count
    return pl.pallas_call(
        functools.partial(last_kernel, length, offsets),
        out_shape=jax.ShapeDtypeStruct(stream.shape, BF16),
        in_specs=[ANY] + [VMEM] * len(pieces),
        out_specs=ANY,
        scratch_shapes=[
            pltpu.VMEM((count, rows, columns), BF16),
            pltpu.VMEM((count, rows, columns), BF16),
            pltpu.SemaphoreType.DMA((count,)),
            pltpu.SemaphoreType.DMA((count,)),
        ],
        input_output_aliases={0: 0},
        name="finish_last",
    )(stream, *pieces)


def on_device(
    length,
    ring,
    skip_stream_vector,
    probe_preactivation,
    retention_preactivation,
    content_vector,
    emission_preactivation,
    retention_slack,
    surge_rate,
    subspace_scaling_factor,
    emission_matrix,
    mlp_scaling_factor,
    switch_matrix,
    expansion_matrix,
    contraction_matrix,
):
    width = probe_preactivation.shape[1]
    heads = width // HEAD_DIM
    side = lax.axis_index("si")
    cross = lax.axis_index("to")
    core = lax.axis_index("ti")
    shifts = [(dx, dy) for dx in range(ring) for dy in range(2)]
    order = arrivals(length)
    down_groups = groups_of(length)

    def swapped(a):
        pairs = [(2 * y + c, 2 * c + y) for y in range(2) for c in range(2)]
        return lax.ppermute(a, ("si", "ti"), pairs)

    def traded(a, dx, dy):
        pairs = [
            ((y * ring + x) * 2 + c, ((c ^ dy) * ring + (x + dx) % ring) * 2 + y)
            for y in range(2)
            for x in range(ring)
            for c in range(2)
        ]
        return lax.ppermute(a, ("si", "to", "ti"), pairs)

    def returned(a, dx, dy):
        pairs = [
            (((c ^ dy) * ring + (x + dx) % ring) * 2 + y, (y * ring + x) * 2 + c)
            for y in range(2)
            for x in range(ring)
            for c in range(2)
        ]
        return lax.ppermute(a, ("si", "to", "ti"), pairs)

    def dealt(a, dx, dc):
        pairs = [
            (2 * x + c, 2 * ((x + dx) % ring) + (c ^ dc)) for x in range(ring) for c in range(2)
        ]
        return lax.ppermute(a, ("to", "ti"), pairs)

    def twin(a):
        return lax.ppermute(a, "ti", [(0, 1), (1, 0)])

    def spread(a, held=None):
        blocks = [a] * length
        for step in range(1, length // 2 + 1):
            if step == 1 and held is not None:
                pairs = [
                    ((i * 2 + y) * 2 + c, ((i + 1) % length * 2 + c) * 2 + y)
                    for i in range(length)
                    for y in range(2)
                    for c in range(2)
                ]
                blocks[step] = lax.ppermute(held, ("so", "si", "ti"), pairs)
                continue
            pairs = [(i, (i + 1) % length) for i in range(length)]
            blocks[step] = lax.ppermute(blocks[step - 1], "so", pairs)
        for step in range(1, (length - 1) // 2 + 1):
            pairs = [((i + 1) % length, i) for i in range(length)]
            source = blocks[(length - step + 1) % length]
            blocks[length - step] = lax.ppermute(source, "so", pairs)
        return blocks

    gates = spread(swapped(switch_matrix), switch_matrix)
    ups = spread(swapped(expansion_matrix))
    downs = spread(swapped(contraction_matrix))

    out, carried, message = local_scan(
        probe_preactivation,
        retention_preactivation,
        content_vector,
        retention_slack,
        surge_rate,
    )

    def opened(a):
        a = a.astype(F32)
        return a[:width].reshape(heads, HEAD_DIM, HEAD_DIM), a[width : width + heads][:, None, :]

    def closed(state, decay):
        return jnp.concatenate(
            [
                state.reshape(width, HEAD_DIM),
                decay.reshape(heads, HEAD_DIM),
                jnp.zeros((16 - heads, HEAD_DIM), F32),
            ]
        ).astype(BF16)

    other = lax.ppermute(message, "si", [(0, 1), (1, 0)])
    first_state, first_decay = opened(jnp.where(side == 0, message, other))
    second_state, second_decay = opened(jnp.where(side == 0, other, message))
    plane = closed(second_decay * first_state + second_state, first_decay * second_decay)
    incoming = jnp.zeros_like(first_state)
    weight = jnp.ones_like(first_decay)
    for k in range(1, length):
        pairs = [(i, i + k) for i in range(length - k)]
        state, decay = opened(lax.ppermute(plane, "so", pairs))
        incoming = incoming + weight * state
        weight = weight * decay
    incoming = jnp.where(side == 0, incoming, first_decay * incoming + first_state)
    came = [lax.rem(cross - dx + ring, ring) * 2 + (core ^ dc) for dx, dc in shifts]
    goes = [lax.rem(cross + dx, ring) * 2 + (core ^ dc) for dx, dc in shifts]
    mixed = mix(
        out,
        carried,
        incoming.reshape(width, HEAD_DIM),
        emission_preactivation,
        subspace_scaling_factor,
        jnp.stack(goes).astype(jnp.int32),
    )
    mixed = [mixed[0]] + [dealt(mixed[index], *shifts[index]) for index in range(1, len(shifts))]
    stream, normed = project(
        mixed,
        jnp.stack(came).astype(jnp.int32),
        emission_matrix,
        skip_stream_vector,
        mlp_scaling_factor,
    )
    normed = [traded(normed, dx, dy) for dx, dy in shifts]

    gates = [gates[offset] for offset in order]
    ups = [ups[offset] for offset in order]
    packed = pack(gates[:-1] + ups[:-1])
    packed = twin(packed)
    down_twins = [twin(block) for block in downs]
    last_twins = twin(gates[-1]), twin(ups[-1])
    hidden, *first = make_hidden(normed, gates, ups, packed, *last_twins, downs[0], down_twins[0])

    pieces = []
    for group, offsets in enumerate(down_groups):
        if group:
            blocks = [b for k in offsets for b in (downs[k], down_twins[k])]
            first = down(hidden, blocks, len(shifts))
        for index, (dx, dy) in enumerate(shifts):
            pieces.append(returned(first[index], dx, dy))
    earlier = len(shifts) * (len(down_groups) - 1)
    stream = finish(stream, pieces[:earlier], down_groups[:-1], length, len(shifts))
    return finish_last(stream, pieces[earlier:], down_groups[-1], length)


def groups_of(length):
    order = arrivals(length)
    return (order[:1], order[1:-1], order[-1:])


def solution(mesh):
    length, ring = mesh.shape["sp"] // 2, mesh.shape["tp"] // 2
    split = Mesh(mesh.devices.reshape(length, 2, ring, 2), ("so", "si", "to", "ti"))
    sp, tp = ("so", "si"), ("to", "ti")
    in_specs = (
        P(sp + tp, None),
        P(sp, tp),
        P(sp, tp),
        P(sp, tp),
        P(sp, tp),
        P(tp),
        P(sp, tp),
        P(tp),
        P(),
        P(),
        P(sp, tp),
        P(sp, tp),
        P(tp, sp),
    )


    def body(*arguments):
        return on_device(length, ring, *arguments)

    return jax.shard_map(
        body, mesh=split, in_specs=in_specs, out_specs=P(sp + tp, None), check_vma=False
    )
```

```python
import functools

import jax
import jax.numpy as jnp
from jax import lax
from jax.experimental import pallas as pl
from jax.experimental.pallas import tpu as pltpu
from jax.sharding import Mesh
from jax.sharding import PartitionSpec as P


HEAD_DIM = 128
BLOCK = 64
CHUNK = 512
SPAN = 256
ROOM = 67_000_000
EPSILON = 1e-06
F32 = jnp.float32
BF16 = jnp.bfloat16
ANY = pl.BlockSpec(memory_space=pltpu.HBM)
VMEM = pl.BlockSpec(memory_space=pltpu.VMEM)


NN = (((1,), (0,)), ((), ()))
NT = (((1,), (1,)), ((), ()))
TN = (((0,), (0,)), ((), ()))


def dot(a, b, dims=NN):
    return lax.dot_general(a, b, dims, preferred_element_type=F32)


def parts(a):
    high = a.astype(BF16)
    return high, (a - high.astype(F32)).astype(BF16)


def dot_split(a, b, dims):
    a_high, a_low = parts(a)
    b_high, b_low = parts(b)
    return dot(a_high, b_high, dims) + (dot(a_high, b_low, dims) + dot(a_low, b_high, dims))


def exact_sums(ones, rate):
    high = rate.astype(BF16)
    rest = rate - high.astype(F32)
    middle = rest.astype(BF16)
    low = (rest - middle.astype(F32)).astype(BF16)
    return dot(ones, high) + (dot(ones, middle) + dot(ones, low))


def state_kernel(retention, content, slack, surge, message, state, offset):
    rows, width = retention.shape
    heads = width // HEAD_DIM
    span = min(SPAN, rows)
    first = lax.broadcasted_iota(jnp.int32, (span, span), 0)
    second = lax.broadcasted_iota(jnp.int32, (span, span), 1)
    later = jnp.where(second > first, 1.0, 0.0).astype(BF16)
    state[...] = jnp.zeros_like(state)
    offset[...] = jnp.zeros_like(offset)
    for turn in range(rows // span):
        here = slice(turn * span, (turn + 1) * span)
        gate = slack[...] * jax.nn.sigmoid(-retention[here, :].astype(F32))
        rate = jnp.log1p(-gate) + surge[here, :]
        following = exact_sums(later, rate)
        leave_high, leave_low = parts(gate * jnp.exp(following))
        total = following[0:1, :] + rate[0:1, :]
        decay = jnp.exp(total)
        for head in range(heads):
            lanes = slice(head * HEAD_DIM, (head + 1) * HEAD_DIM)
            values = content[here, lanes]
            state[lanes, :] = decay[:, lanes] * state[lanes, :] + (
                dot(values, leave_high[:, lanes], TN) + dot(values, leave_low[:, lanes], TN)
            )
        offset[...] += total
    message[0:width, :] = state[...].astype(BF16)
    final = jnp.exp(offset[...])
    tail = jnp.concatenate(
        [final[:, h * HEAD_DIM : (h + 1) * HEAD_DIM] for h in range(heads)]
        + [jnp.zeros((16 - heads, HEAD_DIM), F32)],
        axis=0,
    )
    message[width : width + 16, :] = tail.astype(BF16)


def passed_on(retention, content, slack, surge):
    width = retention.shape[1]
    return pl.pallas_call(
        state_kernel,
        out_shape=jax.ShapeDtypeStruct((width + 16, HEAD_DIM), BF16),
        in_specs=[VMEM] * 4,
        out_specs=VMEM,
        scratch_shapes=[pltpu.VMEM((width, HEAD_DIM), F32), pltpu.VMEM((1, width), F32)],
        name="passed_on",
    )(retention, content, slack.reshape(1, width), surge)


def scan_kernel(probe, retention, content, slack, surge, out, carried, state, offset):
    rows, width = probe.shape
    heads = width // HEAD_DIM
    state[...] = jnp.zeros_like(state)
    offset[...] = jnp.zeros_like(offset)
    first = lax.broadcasted_iota(jnp.int32, (BLOCK, BLOCK), 0)
    second = lax.broadcasted_iota(jnp.int32, (BLOCK, BLOCK), 1)
    causal = first >= second
    ones = jnp.where(causal, 1.0, 0.0).astype(BF16)

    def step(turn, _):
        here = pl.ds(pl.multiple_of(turn * BLOCK, BLOCK), BLOCK)
        before = probe[here, :].astype(F32)
        query = before * jax.nn.sigmoid(before)
        gate = slack[...] * jax.nn.sigmoid(-retention[here, :].astype(F32))
        rate = jnp.log1p(-gate) + surge[here, :]
        value = content[here, :]
        cumulative = exact_sums(ones, rate)
        middle = cumulative[BLOCK // 2 : BLOCK // 2 + 1, :]
        total = cumulative[BLOCK - 1 : BLOCK, :]
        left = query * jnp.exp(cumulative - middle)
        right = gate * jnp.exp(middle - cumulative)
        entering = query * jnp.exp(cumulative)
        leaving = gate * jnp.exp(total - cumulative)
        carried[here, :] = query * jnp.exp(cumulative + offset[...])
        decay = jnp.exp(total)
        for head in range(heads):
            lanes = slice(head * HEAD_DIM, (head + 1) * HEAD_DIM)
            scores = jnp.where(causal, dot_split(left[:, lanes], right[:, lanes], NT), 0.0)
            score_high, score_low = parts(scores)
            held = state[lanes, :]
            values = value[:, lanes]
            out[here, lanes] = dot_split(entering[:, lanes], held, NT) + (
                dot(score_high, values) + dot(score_low, values)
            )
            leave_high, leave_low = parts(leaving[:, lanes])
            state[lanes, :] = decay[:, lanes] * held + (
                dot(values, leave_high, TN) + dot(values, leave_low, TN)
            )
        offset[...] += total
        return 0

    lax.fori_loop(0, rows // BLOCK, step, 0, unroll=4)


def local_scan(probe, retention, content, slack, surge):
    rows, width = probe.shape
    return pl.pallas_call(
        scan_kernel,
        out_shape=(
            jax.ShapeDtypeStruct((rows, width), F32),
            jax.ShapeDtypeStruct((rows, width), F32),
        ),
        in_specs=[VMEM] * 5,
        out_specs=(VMEM, VMEM),
        scratch_shapes=[pltpu.VMEM((width, HEAD_DIM), F32), pltpu.VMEM((1, width), F32)],
        name="local_scan",
    )(probe, retention, content, slack.reshape(1, width), surge)


def mix_kernel(order, out, carried, state, emission, gain, *pieces):
    for head in range(out.shape[1] // HEAD_DIM):
        lanes = slice(head * HEAD_DIM, (head + 1) * HEAD_DIM)
        whole = out[:, lanes] + dot_split(carried[:, lanes], state[lanes, :], NT)
        squares = jnp.mean(whole * whole, axis=-1, keepdims=True)
        before = emission[:, lanes].astype(F32)
        scaled = whole * lax.rsqrt(squares + EPSILON) * gain[:, lanes]
        mixed = (scaled * (before * jax.nn.sigmoid(before))).astype(BF16)
        for index, piece in enumerate(pieces):

            @pl.when(pl.program_id(0) == index)
            def _(piece=piece):
                piece[:, lanes] = mixed


def mix(out, carried, state, emission, gain, order):
    rows, width = out.shape
    count = order.shape[0]
    tile = rows // count
    row_spec = pl.BlockSpec((tile, width), lambda i, o: (o[i], 0))
    return pl.pallas_call(
        mix_kernel,
        grid_spec=pltpu.PrefetchScalarGridSpec(
            num_scalar_prefetch=1,
            grid=(count,),
            in_specs=[
                row_spec,
                row_spec,
                pl.BlockSpec((width, HEAD_DIM), lambda i, o: (0, 0)),
                row_spec,
                pl.BlockSpec((1, width), lambda i, o: (0, 0)),
            ],
            out_specs=[pl.BlockSpec((tile, width), lambda i, o: (0, 0))] * count,
        ),
        out_shape=[jax.ShapeDtypeStruct((tile, width), BF16)] * count,
        name="mix",
    )(order, out, carried, state, emission, gain.reshape(1, width))


def project_kernel(count, order, *refs):
    mixed, (weight, skip, gain, stream, normed) = refs[:count], refs[count:]
    width = mixed[0].shape[1]
    total = None
    for index in range(count):
        rows = pl.ds(pl.multiple_of(order[index] * width, width), width)
        term = dot(mixed[index][...], weight[rows, :])
        total = term if total is None else total + term
    added = (skip[...].astype(F32) + total).astype(BF16)
    stream[...] = added
    wide = added.astype(F32)
    squares = jnp.mean(wide * wide, axis=-1, keepdims=True)
    normed[...] = (wide * lax.rsqrt(squares + EPSILON) * gain[...]).astype(BF16)


def project(mixed, order, weight, skip, gain):
    count = len(mixed)
    shape = jax.ShapeDtypeStruct(skip.shape, BF16)
    return pl.pallas_call(
        functools.partial(project_kernel, count),
        in_specs=[pl.BlockSpec(memory_space=pltpu.SMEM)] + [VMEM] * (count + 3),
        out_specs=(VMEM, VMEM),
        out_shape=(shape, shape),
        name="project",
    )(order, *mixed, weight, skip, gain.reshape(1, -1))


def arrivals(length):
    offsets = [0]
    for step in range(1, length // 2 + 1):
        offsets += [step, length - step][: min(2, length - len(offsets))]
    return offsets


def column_place(line, offset, length):
    return lax.rem(line - offset + length, length)


def hidden_kernel(length, count, own_normed, *refs):
    normed, refs = refs[:count], refs[count:]
    gates, ups, refs = refs[: 2 * length], refs[2 * length : 4 * length], refs[4 * length :]
    (down_own, down_twin), refs = refs[:2], refs[2:]
    hidden, outs, refs = refs[0], refs[1 : 1 + count], refs[1 + count :]
    rows_now, gate_all, up_all, down_all, gate_sum, up_sum, sems, piece_sem = refs
    depth, units = gates[0].shape
    columns = down_own.shape[1]
    line = lax.axis_index("so")
    core = lax.axis_index("ti")
    turn = pl.program_id(0)

    height = normed[0].shape[0]
    group = hidden.shape[0] // height
    half = length * depth

    places = []
    weight_copies = []
    for twin in range(2):
        side = 1 - core if twin else core
        for index, offset in enumerate(arrivals(length)):
            slot = twin * length + index
            gate_block, up_block = gates[slot], ups[slot]
            if gate_block.shape[0] > depth:
                gate_block = gate_block.at[pl.ds(0, depth), :]
                up_block = up_block.at[pl.ds(depth, depth), :]
            rows = pl.ds(slot * depth, depth)
            weight_copies += [
                pltpu.make_async_copy(gate_block, gate_all.at[rows, :], sems.at[2 * slot]),
                pltpu.make_async_copy(up_block, up_all.at[rows, :], sems.at[2 * slot + 1]),
            ]
            places.append(2 * column_place(line, offset, length) + side)
    down_copies = [
        pltpu.make_async_copy(
            block, down_all.at[:, pl.ds(index * columns, columns)], sems.at[4 * length + index]
        )
        for index, block in enumerate((down_own, down_twin))
    ]

    def piece_copies(piece, source=None):
        source = normed[piece] if source is None else source
        return [
            pltpu.make_async_copy(
                source.at[:, pl.ds(pl.multiple_of(place * depth, depth), depth)],
                rows_now.at[pl.ds(piece * height, height), pl.ds(slot * depth, depth)],
                piece_sem.at[piece * 2 * length + slot],
            )
            for slot, place in enumerate(places)
        ]

    chunks = [slice(start, min(start + CHUNK, units)) for start in range(0, units, CHUNK)]

    @pl.when(turn == 0)
    def _():
        stays = lax.axis_index("si") == core

        @pl.when(stays)
        def _():
            for copy in piece_copies(0, own_normed):
                copy.start()

        @pl.when(jnp.logical_not(stays))
        def _():
            for copy in piece_copies(0):
                copy.start()

        first = [copy for piece in range(group) for copy in piece_copies(piece)]
        others = [copy for piece in range(group, count) for copy in piece_copies(piece)]
        for copy in first[2 * length :] + weight_copies + down_copies + others:
            copy.start()
        for copy in first + weight_copies[: 2 * length]:
            copy.wait()
        now = slice(0, group * height)
        for lanes in chunks:
            gate_sum[:, lanes] = dot(rows_now[now, :half], gate_all[:half, lanes])
            up_sum[:, lanes] = dot(rows_now[now, :half], up_all[:half, lanes])
        for copy in weight_copies[2 * length :]:
            copy.wait()
        for lanes in chunks:
            gate = gate_sum[:, lanes] + dot(rows_now[now, half:], gate_all[half:, lanes])
            up = up_sum[:, lanes] + dot(rows_now[now, half:], up_all[half:, lanes])
            hidden[:, lanes] = (gate * jax.nn.sigmoid(gate) * up).astype(BF16)
        for copy in down_copies:
            copy.wait()

    for piece in range(group, count):

        @pl.when(turn == piece // group)
        def _(piece=piece):
            for copy in piece_copies(piece):
                copy.wait()

    @pl.when(turn > 0)
    def _():
        here = pl.ds(pl.multiple_of(turn * group * height, group * height), group * height)
        for lanes in chunks:
            gate = dot(rows_now[here, :], gate_all[:, lanes])
            up = dot(rows_now[here, :], up_all[:, lanes])
            hidden[:, lanes] = (gate * jax.nn.sigmoid(gate) * up).astype(BF16)

    share = dot(hidden[...], down_all[...]).astype(BF16)
    for index in range(count):

        @pl.when(turn == index // group)
        def _(index=index):
            start = index % group * height
            outs[index][...] = share[start : start + height, :]


def make_hidden(own_normed, normed, gates, ups, down_own, down_twin):
    rows, features = normed[0].shape
    length = len(gates) // 2
    units = gates[0].shape[1]
    columns = 2 * down_own.shape[1]
    count = len(normed)
    return pl.pallas_call(
        functools.partial(hidden_kernel, length, count),
        grid=(count // 2,),
        out_shape=[jax.ShapeDtypeStruct((count * rows, units), BF16)]
        + [jax.ShapeDtypeStruct((rows, columns), BF16)] * count,
        in_specs=[ANY] * (1 + count + 4 * length + 2),
        out_specs=[pl.BlockSpec((2 * rows, units), lambda i: (i, 0))]
        + [pl.BlockSpec((rows, columns), lambda i: (0, 0))] * count,
        scratch_shapes=[
            pltpu.VMEM((count * rows, features), BF16),
            pltpu.VMEM((features, units), BF16),
            pltpu.VMEM((features, units), BF16),
            pltpu.VMEM((units, columns), BF16),
            pltpu.VMEM((2 * rows, units), F32),
            pltpu.VMEM((2 * rows, units), F32),
            pltpu.SemaphoreType.DMA((4 * length + 2,)),
            pltpu.SemaphoreType.DMA((2 * length * count,)),
        ],
        compiler_params=pltpu.CompilerParams(vmem_limit_bytes=ROOM),
        name="make_hidden",
    )(own_normed, *normed, *gates, *ups, down_own, down_twin)


def down_kernel(count, blocks, hidden, *refs):
    weights, outs, (weight, sems) = refs[:blocks], refs[blocks : blocks + count], refs[-2:]
    columns = weights[0].shape[1]
    rows = outs[0].shape[0]
    copies = [
        pltpu.make_async_copy(
            block, weight.at[:, pl.ds(index * columns, columns)], sems.at[index]
        )
        for index, block in enumerate(weights)
    ]
    for copy in copies:
        copy.start()
    for copy in copies:
        copy.wait()
    for index in range(count):
        here = hidden[index * rows : (index + 1) * rows, :]
        outs[index][...] = dot(here, weight[...]).astype(BF16)


def down(hidden, blocks, count):
    rows, units = hidden.shape
    width = len(blocks) * blocks[0].shape[1]
    return pl.pallas_call(
        functools.partial(down_kernel, count, len(blocks)),
        out_shape=[jax.ShapeDtypeStruct((rows // count, width), BF16)] * count,
        in_specs=[VMEM] + [ANY] * len(blocks),
        out_specs=[VMEM] * count,
        scratch_shapes=[
            pltpu.VMEM((units, width), BF16),
            pltpu.SemaphoreType.DMA((len(blocks),)),
        ],
        name="down",
    )(hidden, *blocks)


def summed(pieces, lanes):
    stays = lax.axis_index("si") == lax.axis_index("ti")
    total = jnp.where(stays, pieces[0][:, lanes].astype(F32), pieces[1][:, lanes].astype(F32))
    for piece in pieces[2:]:
        total = total + piece[:, lanes].astype(F32)
    return total


def finish_kernel(length, groups, count, stream, *refs):
    pieces, out = refs[:-1], refs[-1]
    columns = stream.shape[1] // (2 * length)
    line = lax.axis_index("so")
    side = lax.axis_index("si")
    for group, offsets in enumerate(groups):
        mine = pieces[group * (count + 1) : (group + 1) * (count + 1)]
        for index, offset in enumerate(offsets):
            for twin in range(2):
                place = column_place(line, offset, length)
                block = 2 * place + (1 - side if twin else side)
                lanes = pl.ds(pl.multiple_of(block * columns, columns), columns)
                start = (2 * index + twin) * columns
                local = slice(start, start + columns)
                total = summed(mine, local)
                out[:, lanes] = (stream[:, lanes].astype(F32) + total).astype(BF16)


def finish(stream, pieces, groups, length, count):
    def kernel(stream_ref, *refs):
        refs[-1][...] = stream_ref[...]
        finish_kernel(length, groups, count, stream_ref, *refs)

    return pl.pallas_call(
        kernel,
        out_shape=jax.ShapeDtypeStruct(stream.shape, BF16),
        in_specs=[VMEM] * (1 + len(pieces)),
        out_specs=VMEM,
        name="finish",
    )(stream, *pieces)


def last_kernel(length, offsets, stream, *refs):
    pieces, (out, held, done, read_sems, write_sems) = refs[:-5], refs[-5:]
    columns = held.shape[2]
    line = lax.axis_index("so")
    side = lax.axis_index("si")
    moves = []
    for index, offset in enumerate(offsets):
        for twin in range(2):
            block = 2 * column_place(line, offset, length) + (1 - side if twin else side)
            lanes = pl.ds(pl.multiple_of(block * columns, columns), columns)
            slot = 2 * index + twin
            moves.append(
                (
                    pltpu.make_async_copy(stream.at[:, lanes], held.at[slot], read_sems.at[slot]),
                    pltpu.make_async_copy(done.at[slot], out.at[:, lanes], write_sems.at[slot]),
                )
            )
    for read, _ in moves:
        read.start()
    for slot, (read, write) in enumerate(moves):
        local = slice(slot * columns, (slot + 1) * columns)
        total = summed(pieces, local)
        read.wait()
        done[slot] = (held[slot].astype(F32) + total).astype(BF16)
        write.start()
    for _, write in moves:
        write.wait()


def finish_last(stream, pieces, offsets, length):
    rows = stream.shape[0]
    count = 2 * len(offsets)
    columns = pieces[0].shape[1] // count
    return pl.pallas_call(
        functools.partial(last_kernel, length, offsets),
        out_shape=jax.ShapeDtypeStruct(stream.shape, BF16),
        in_specs=[ANY] + [VMEM] * len(pieces),
        out_specs=ANY,
        scratch_shapes=[
            pltpu.VMEM((count, rows, columns), BF16),
            pltpu.VMEM((count, rows, columns), BF16),
            pltpu.SemaphoreType.DMA((count,)),
            pltpu.SemaphoreType.DMA((count,)),
        ],
        input_output_aliases={0: 0},
        name="finish_last",
    )(stream, *pieces)


def on_device(
    length,
    ring,
    skip_stream_vector,
    probe_preactivation,
    retention_preactivation,
    content_vector,
    emission_preactivation,
    retention_slack,
    surge_rate,
    subspace_scaling_factor,
    emission_matrix,
    mlp_scaling_factor,
    switch_matrix,
    expansion_matrix,
    contraction_matrix,
):
    width = probe_preactivation.shape[1]
    heads = width // HEAD_DIM
    side = lax.axis_index("si")
    cross = lax.axis_index("to")
    core = lax.axis_index("ti")
    shifts = [(dx, dy) for dx in range(ring) for dy in range(2)]
    order = arrivals(length)
    down_groups = groups_of(length)

    def swapped(a):
        pairs = [(2 * y + c, 2 * c + y) for y in range(2) for c in range(2)]
        return lax.ppermute(a, ("si", "ti"), pairs)

    def traded(a, dx, dy):
        pairs = [
            ((y * ring + x) * 2 + c, ((c ^ dy) * ring + (x + dx) % ring) * 2 + y)
            for y in range(2)
            for x in range(ring)
            for c in range(2)
        ]
        pairs = [(source, target) for source, target in pairs if source != target]
        return lax.ppermute(a, ("si", "to", "ti"), pairs)

    def returned(a, dx, dy):
        pairs = [
            (((c ^ dy) * ring + (x + dx) % ring) * 2 + y, (y * ring + x) * 2 + c)
            for y in range(2)
            for x in range(ring)
            for c in range(2)
        ]
        pairs = [(source, target) for source, target in pairs if source != target]
        return lax.ppermute(a, ("si", "to", "ti"), pairs)

    def dealt(a, dx, dc):
        pairs = [
            (2 * x + c, 2 * ((x + dx) % ring) + (c ^ dc)) for x in range(ring) for c in range(2)
        ]
        return lax.ppermute(a, ("to", "ti"), pairs)

    def twin(a):
        return lax.ppermute(a, "ti", [(0, 1), (1, 0)])

    def spread(a, held=None):
        blocks = [a] * length
        for step in range(1, length // 2 + 1):
            if step == 1 and held is not None:
                pairs = [
                    ((i * 2 + y) * 2 + c, ((i + 1) % length * 2 + c) * 2 + y)
                    for i in range(length)
                    for y in range(2)
                    for c in range(2)
                ]
                blocks[step] = lax.ppermute(held, ("so", "si", "ti"), pairs)
                continue
            pairs = [(i, (i + 1) % length) for i in range(length)]
            blocks[step] = lax.ppermute(blocks[step - 1], "so", pairs)
        for step in range(1, (length - 1) // 2 + 1):
            pairs = [((i + 1) % length, i) for i in range(length)]
            source = blocks[(length - step + 1) % length]
            blocks[length - step] = lax.ppermute(source, "so", pairs)
        return blocks

    gates = spread(swapped(switch_matrix), switch_matrix)
    ups = spread(swapped(expansion_matrix))
    moved = lax.ppermute(contraction_matrix, ("si", "ti"), [(1, 2), (2, 1)])
    downs = spread(jnp.where(side == core, contraction_matrix, moved))

    message = passed_on(retention_preactivation, content_vector, retention_slack, surge_rate)
    out, carried = local_scan(
        probe_preactivation,
        retention_preactivation,
        content_vector,
        retention_slack,
        surge_rate,
    )

    def opened(a):
        a = a.astype(F32)
        return a[:width].reshape(heads, HEAD_DIM, HEAD_DIM), a[width : width + heads][:, None, :]

    def closed(state, decay):
        return jnp.concatenate(
            [
                state.reshape(width, HEAD_DIM),
                decay.reshape(heads, HEAD_DIM),
                jnp.zeros((16 - heads, HEAD_DIM), F32),
            ]
        ).astype(BF16)

    other = lax.ppermute(message, "si", [(0, 1), (1, 0)])
    first_state, first_decay = opened(jnp.where(side == 0, message, other))
    second_state, second_decay = opened(jnp.where(side == 0, other, message))
    plane = closed(second_decay * first_state + second_state, first_decay * second_decay)
    incoming = jnp.zeros_like(first_state)
    weight = jnp.ones_like(first_decay)
    for k in range(1, length):
        pairs = [(i, i + k) for i in range(length - k)]
        state, decay = opened(lax.ppermute(plane, "so", pairs))
        incoming = incoming + weight * state
        weight = weight * decay
    incoming = jnp.where(side == 0, incoming, first_decay * incoming + first_state)
    came = [lax.rem(cross - dx + ring, ring) * 2 + (core ^ dc) for dx, dc in shifts]
    goes = [lax.rem(cross + dx, ring) * 2 + (core ^ dc) for dx, dc in shifts]
    mixed = mix(
        out,
        carried,
        incoming.reshape(width, HEAD_DIM),
        emission_preactivation,
        subspace_scaling_factor,
        jnp.stack(goes).astype(jnp.int32),
    )
    mixed = [mixed[0]] + [dealt(mixed[index], *shifts[index]) for index in range(1, len(shifts))]
    stream, normed = project(
        mixed,
        jnp.stack(came).astype(jnp.int32),
        emission_matrix,
        skip_stream_vector,
        mlp_scaling_factor,
    )
    own_normed = normed
    normed = [traded(normed, dx, dy) for dx, dy in shifts]

    both = twin(jnp.concatenate([gates[0], ups[0]]))
    later = order[1:]
    gates = [gates[k] for k in order] + [both] + [twin(gates[k]) for k in later]
    ups = [ups[k] for k in order] + [both] + [twin(ups[k]) for k in later]
    down_twins = [twin(block) for block in downs]
    hidden, *first = make_hidden(own_normed, normed, gates, ups, downs[0], down_twins[0])

    pieces = []
    for group, offsets in enumerate(down_groups):
        if group:
            blocks = [b for k in offsets for b in (downs[k], down_twins[k])]
            first = down(hidden, blocks, len(shifts))
        pieces.append(first[0])
        for index, (dx, dy) in enumerate(shifts):
            pieces.append(returned(first[index], dx, dy))
    earlier = (len(shifts) + 1) * (len(down_groups) - 1)
    stream = finish(stream, pieces[:earlier], down_groups[:-1], length, len(shifts))
    return finish_last(stream, pieces[earlier:], down_groups[-1], length)


def groups_of(length):
    order = arrivals(length)
    return (order[:1], order[1:-1], order[-1:])


def solution(mesh):
    length, ring = mesh.shape["sp"] // 2, mesh.shape["tp"] // 2
    split = Mesh(mesh.devices.reshape(length, 2, ring, 2), ("so", "si", "to", "ti"))
    sp, tp = ("so", "si"), ("to", "ti")
    in_specs = (
        P(sp + tp, None),
        P(sp, tp),
        P(sp, tp),
        P(sp, tp),
        P(sp, tp),
        P(tp),
        P(sp, tp),
        P(tp),
        P(),
        P(),
        P(sp, tp),
        P(sp, tp),
        P(tp, sp),
    )


    def body(*arguments):
        return on_device(length, ring, *arguments)

    return jax.shard_map(
        body, mesh=split, in_specs=in_specs, out_specs=P(sp + tp, None), check_vma=False
    )
```
